32 devices in a mesh: sp: 16 (over z, y, x), tp: 2 (over core).
Axes of the slice: x: 2, y: 2, z: 4, core: 2. Of those that a mesh axis runs over, the one named last changes fastest.
Arguments:
- prompt: bfloat16 [8, 1024, 2048], P(None, 'sp'), may hold values from -6 to 6
- keep_scale: float32 [8, 1024], P(None, 'sp'), may hold values from 0.25 to 1
- new_token: bfloat16 [8, 2048], P(None, 'tp'), may hold values from -6 to 6
- w_query: bfloat16 [2048, 1024], P(None, 'tp'), may hold values from -0.125 to 0.125
- w_forget: bfloat16 [2048, 1024], P(None, 'tp'), may hold values from -0.125 to 0.125
- w_value: bfloat16 [2048, 1024], P(None, 'tp'), may hold values from -2.109375 to 2.109375
- w_outgate: bfloat16 [2048, 1024], P(None, 'tp'), may hold values from -0.125 to 0.125
- floor_gap: float32 [1024], P('tp'), may hold values from 0 to 0.06
- norm_gain: float32 [128], replicated, may hold values from 0.1 to 1.9
Outputs:
- state_cache: bfloat16 [8, 1024, 128], P('tp', 'sp')
- first_read: bfloat16 [8, 1024], P(None, 'tp')
The draws below stay inside these ranges and needn't reach their ends.
All inputs are finite; a program needn't handle non-finite values.
Results may differ from the reference program's by a relative error of at most 0.0022.
The reference program's roundings to bfloat16 on the way (of `values` and `new_value`) count: a program that leaves them out, or rounds other values in their place, can miss the bound.
Values may be sent and summed in bfloat16 or wider, within the bound.
A program may use at most 64 MiB of HBM per device.

```python
import math
import jax
import jax.numpy as jnp
from jax import lax

D = 2048
HEADS = 8
HEAD_DIM = 128
MIX_WIDTH = 1024
PROMPT_COUNT = 8
TOK_SEQ = 64
PROMPT_LENGTH = 1024


def draw_keep_scale(key, part):
    key_rate = jax.random.fold_in(key, 11)
    key_positions = jax.random.fold_in(key, 12)
    key_depth = jax.random.fold_in(key, 13)
    blocks = PROMPT_LENGTH // TOK_SEQ
    block_rate = jnp.exp(jax.random.uniform(key_rate, (PROMPT_COUNT, blocks, 1), minval=math.log(0.4), maxval=math.log(1.6))) / PROMPT_LENGTH
    steady = jnp.broadcast_to(jnp.exp(-block_rate), (PROMPT_COUNT, blocks, TOK_SEQ)).reshape(PROMPT_COUNT, PROMPT_LENGTH)
    spike_positions = jax.random.randint(key_positions, (PROMPT_COUNT, 2), 0, PROMPT_LENGTH)
    spike_match = jnp.arange(PROMPT_LENGTH, dtype=jnp.int32)[None, None, :] == spike_positions[:, :, None]
    intensity = jax.random.uniform(key_depth, (PROMPT_COUNT, 2, 1), minval=0.55, maxval=0.8)
    multiplier = jnp.prod(jnp.where(spike_match, intensity, 1.0), axis=1)
    return (steady * multiplier).astype(jnp.float32)


def draw_floor_gap(key, part):
    key_order = jax.random.fold_in(key, 21)
    key_fast = jax.random.fold_in(key, 22)
    key_slow = jax.random.fold_in(key, 23)
    head_order = jax.random.permutation(key_order, HEADS)
    fast_count = HEADS // 2
    fast_head = head_order < fast_count
    fast_gap = jnp.exp(jax.random.uniform(key_fast, (HEADS, HEAD_DIM), minval=math.log(0.02), maxval=math.log(0.06)))
    slow_gap = jnp.exp(jax.random.uniform(key_slow, (HEADS, HEAD_DIM), minval=math.log(0.2), maxval=0.0)) / PROMPT_LENGTH
    return jnp.where(fast_head[:, None], fast_gap, slow_gap).reshape(HEADS * HEAD_DIM).astype(jnp.float32)


def levels(key, extent, split, least, largest):
    factor_of = 1.0
    for position, parts in split:
        steps = jax.random.uniform(jax.random.fold_in(jax.random.fold_in(key, 6), position), (parts,), jnp.float32, least / len(split), largest / len(split))
        factor_of = factor_of * jnp.repeat(jnp.exp(steps), extent[position] // parts).reshape((-1,) + (1,) * (len(extent) - 1 - position))
    return factor_of


def normal_values(key, dims, deviation, most, split=(), kind=jnp.bfloat16):
    values = jax.random.normal(key, dims, jnp.float32) * deviation
    if len(split) > 0:
        values = levels(key, dims, split, -0.22, 0.18) * values
    return jnp.clip(values, min=-most, max=most).astype(kind)


def setup_inputs(seed: int = 0) -> dict:
    splits = jax.random.split(jax.random.key(seed), 10)
    return {
        "prompt": normal_values(splits[0], (PROMPT_COUNT, PROMPT_LENGTH, D), 1.0, 6.0, ((1, 16),)),
        "keep_scale": draw_keep_scale(jax.random.fold_in(splits[9], 71), 0),
        "new_token": normal_values(splits[2], (PROMPT_COUNT, D), 1.0, 6.0, ((1, 2),)),
        "w_query": normal_values(splits[3], (D, MIX_WIDTH), D ** -0.5, 0.125, ((1, 2),)),
        "w_forget": normal_values(splits[4], (D, MIX_WIDTH), D ** -0.5, 0.125, ((1, 2),)),
        "w_value": normal_values(splits[5], (D, MIX_WIDTH), (0.5 * PROMPT_LENGTH ** 0.5 * D ** -0.5), 2.109375, ((1, 2),)),
        "w_outgate": normal_values(splits[6], (D, MIX_WIDTH), D ** -0.5, 0.125, ((1, 2),)),
        "floor_gap": draw_floor_gap(jax.random.fold_in(splits[9], 71), 0),
        "norm_gain": jnp.clip(1.0 + 0.18 * jax.random.normal(splits[8], (HEAD_DIM,), jnp.float32), 0.1, 1.9),
    }


EPSILON = 1e-06

def reference(prompt, keep_scale, new_token, w_query, w_forget, w_value, w_outgate, floor_gap, norm_gain):
    floor_rows = floor_gap.reshape(HEADS, HEAD_DIM)

    def one_sequence(inputs):
        seq_rows, keep_row = inputs
        forget_pre = jnp.dot(seq_rows, w_forget, preferred_element_type=jnp.float32).reshape(PROMPT_LENGTH, HEADS, HEAD_DIM)
        values = jnp.dot(seq_rows, w_value, preferred_element_type=jnp.float32).astype(jnp.bfloat16)
        values = lax.optimization_barrier(values).astype(jnp.float32).reshape(PROMPT_LENGTH, HEADS, HEAD_DIM)
        forget_loss = floor_rows * (1.0 - jax.nn.sigmoid(forget_pre))
        keep_factor = keep_row[:, None, None]
        log_forget = jnp.log(keep_factor) + jnp.log1p(-forget_loss)
        input_gate = 1.0 - keep_factor + keep_factor * forget_loss
        later_log = lax.cumsum(log_forget, axis=0, reverse=True) - log_forget
        return jnp.einsum('thc,thv->hcv', input_gate * jnp.exp(later_log), values, precision=lax.Precision.HIGHEST)
    final_state = lax.map(one_sequence, (prompt, keep_scale))
    state_cache = final_state.transpose(1, 0, 2, 3).reshape(HEADS, PROMPT_COUNT * HEAD_DIM, HEAD_DIM).astype(jnp.bfloat16)
    shaped = (PROMPT_COUNT, HEADS, HEAD_DIM)
    query = jnp.dot(new_token, w_query, preferred_element_type=jnp.float32).reshape(shaped)
    new_forget = jnp.dot(new_token, w_forget, preferred_element_type=jnp.float32).reshape(shaped)
    new_gate = jnp.dot(new_token, w_outgate, preferred_element_type=jnp.float32).reshape(shaped)
    new_value = jnp.dot(new_token, w_value, preferred_element_type=jnp.float32).astype(jnp.bfloat16)
    new_value = lax.optimization_barrier(new_value).astype(jnp.float32).reshape(shaped)
    new_loss = floor_rows * (1.0 - jax.nn.sigmoid(new_forget))
    mixed = jnp.einsum('shc,shcv->shv', query * (1.0 - new_loss), final_state, precision=lax.Precision.HIGHEST)
    mixed = mixed + lax.optimization_barrier(jnp.sum(query * new_loss, axis=-1, keepdims=True)) * new_value
    normed = mixed * lax.rsqrt(lax.optimization_barrier(jnp.mean(mixed * mixed, axis=-1, keepdims=True)) + EPSILON)
    first_read = (normed * norm_gain * jax.nn.silu(new_gate)).reshape(PROMPT_COUNT, HEADS * HEAD_DIM).astype(jnp.bfloat16)
    return (state_cache, first_read)
```

```python
import functools

import jax
import jax.numpy as jnp
from jax import lax
from jax.experimental import pallas as pl
from jax.experimental.pallas import tpu as pltpu
from jax.sharding import PartitionSpec as P

EPSILON = 1e-06
MESH = pl.DeviceIdType.MESH
F32 = jnp.float32
BF16 = jnp.bfloat16


def partner(mine, step, count):
    total, bit = 0, 1
    while bit < count:
        total = total + bit * lax.rem(lax.rem(mine // bit, 2) + lax.rem(step // bit, 2), 2)
        bit *= 2
    return total


def pieces(x, count):
    out = []
    for _ in range(count):
        piece = x.astype(BF16)
        out.append(piece)
        x = x - piece.astype(F32)
    return out


def arrival_order(members):
    if members == 8:
        return (0, 7, 3, 4, 5, 2, 6, 1)
    return (0,) + tuple(range(members - 1, 0, -1))


def kernel(
    sizes,
    prompt, keep, token, w_query, w_forget, w_value, w_outgate, floor, gain,
    cache_out, read_out,
    stage, blocks, keeps, tokens, wq, wf, wv, wo, floors, gains,
    weighted, values, logs, suffixes, decays, totals, got_totals, states, got_states, reads, sums,
    local_sem, stage_sem, direct_send, direct_recv, keep_send, keep_recv, fwd_send, fwd_recv,
    token_send, token_recv, total_send, total_recv, row_send, row_recv, state_send, state_recv, read_send, read_recv,
):
    n, t, s_count, members, cubes, heads, head, rows = sizes
    group = cubes
    me, core = lax.axis_index("sp"), lax.axis_index("tp")
    cube, place = me // members, lax.rem(me, members)
    model = prompt.shape[2]
    part = model // t
    positions = prompt.shape[1]
    width = heads * head
    order = arrival_order(members)
    pairs = members // 2
    batches = 2 if heads % 2 == 0 else 1
    batch = heads // batches

    def prompt_of(p):
        if members % 4:
            return p
        low = lax.rem(p, 4)
        return p - low + lax.rem(low, 2) * 2 + low // 2

    def columns(c):
        return pl.ds(pl.multiple_of(c * part, part), part)

    def relation(k):
        if isinstance(k, int):
            return order[k]
        r = 0
        for i, value in enumerate(order):
            r = r + value * jnp.where(k == i, 1, 0)
        return r

    def peer(k):
        return partner(place, relation(k), members)

    mine = prompt_of(place)

    staged = [None] + [
        pltpu.make_async_copy(prompt.at[prompt_of(peer(k)), :, columns(core)], stage.at[k - 1], stage_sem.at[k])
        for k in range(1, members)
    ]
    local = [
        pltpu.make_async_copy(keep, keeps.at[0], local_sem.at[0]),
        pltpu.make_async_copy(token, tokens.at[core], local_sem.at[1]),
        pltpu.make_async_copy(floor, floors, local_sem.at[2]),
        pltpu.make_async_copy(gain, gains, local_sem.at[3]),
        pltpu.make_async_copy(prompt.at[mine], blocks.at[0], local_sem.at[4]),
        pltpu.make_async_copy(w_forget, wf, local_sem.at[5]),
        pltpu.make_async_copy(w_value, wv, local_sem.at[6]),
        pltpu.make_async_copy(w_query, wq, local_sem.at[7]),
        pltpu.make_async_copy(w_outgate, wo, local_sem.at[8]),
    ]

    barrier = pltpu.get_barrier_semaphore()
    for k in range(1, members):
        pl.semaphore_signal(barrier, inc=1, device_id=(cube * members + peer(k), core), device_id_type=MESH)
    for o in range(1, cubes):
        pl.semaphore_signal(barrier, inc=1, device_id=(lax.rem(me + o * members, n), core), device_id_type=MESH)
    for o in range(1, t):
        pl.semaphore_signal(barrier, inc=1, device_id=(me, lax.rem(core + o, t)), device_id_type=MESH)
    local[0].start()
    local[1].start()
    for k in range(1, members):
        staged[k].start()
    for copy in local[2:]:
        copy.start()

    def direct(k):
        return pltpu.make_async_remote_copy(
            src_ref=stage.at[k - 1],
            dst_ref=blocks.at[k, :, columns(core)],
            send_sem=direct_send.at[k], recv_sem=direct_recv.at[k],
            device_id=(cube * members + peer(k), core), device_id_type=MESH,
        )

    def keep_copy(k):
        return pltpu.make_async_remote_copy(
            src_ref=keeps.at[0], dst_ref=keeps.at[k],
            send_sem=keep_send.at[k], recv_sem=keep_recv.at[k],
            device_id=(cube * members + peer(k), core), device_id_type=MESH,
        )

    def forward(k, o, c):
        piece = blocks.at[k, :, columns(c)]
        return pltpu.make_async_remote_copy(
            src_ref=piece, dst_ref=piece,
            send_sem=fwd_send.at[k, o], recv_sem=fwd_recv.at[k, o],
            device_id=(me, lax.rem(core + o, t)), device_id_type=MESH,
        )

    def token_copy(o, c):
        return pltpu.make_async_remote_copy(
            src_ref=tokens.at[c], dst_ref=tokens.at[c],
            send_sem=token_send.at[o], recv_sem=token_recv.at[o],
            device_id=(me, lax.rem(core + o, t)), device_id_type=MESH,
        )

    local[0].wait()
    local[1].wait()
    with jax.named_scope("barrier"):
        pl.semaphore_wait(barrier, members - 1 + cubes - 1 + t - 1)
    for k in range(1, members):
        keep_copy(k).start()
    for k in range(1, members):
        staged[k].wait()
        direct(k).start()
    for o in range(1, t):
        token_copy(o, core).start()

    with jax.named_scope("wlocal"):
        for copy in local[2:]:
            copy.wait()
        for o in range(1, t):
            token_copy(o, lax.rem(core - o + t, t)).wait_recv()
    floor_row = floors[...]

    with jax.named_scope("token"):
        feature = jnp.concatenate([tokens[c] for c in range(t)], axis=1)
        query = jnp.dot(feature, wq[...], preferred_element_type=F32)
        new_forget = jnp.dot(feature, wf[...], preferred_element_type=F32)
        new_value = jnp.dot(feature, wv[...], preferred_element_type=F32).astype(BF16).astype(F32)
        new_gate = jnp.dot(feature, wo[...], preferred_element_type=F32)
        new_loss = floor_row * (1.0 / (1.0 + jnp.exp(new_forget)))
        read_weight = query * (1.0 - new_loss)
        sums[0] = query * new_loss
        sums[1] = new_value
        sums[2] = new_gate * (1.0 / (1.0 + jnp.exp(-new_gate)))
        seq = lax.broadcasted_iota(jnp.int32, read_weight.shape, 0)
        picked = jnp.where(seq == mine, read_weight, 0.0)
        sums[3] = jnp.broadcast_to(jnp.sum(picked, axis=0, keepdims=True), read_weight.shape)

    def block_rows(k, count):
        return blocks[pl.ds(k, count)].reshape(count * positions, model)

    def value(k, count):
        out = jnp.dot(block_rows(k, count), wv[...], preferred_element_type=F32).astype(BF16)
        values[pl.ds(k, count)] = out.reshape(count, positions, width)

    def forget(k, count):
        size = count * positions
        pre = jnp.dot(block_rows(k, count), wf[...], preferred_element_type=F32)
        loss = floor_row * (1.0 / (1.0 + jnp.exp(pre)))
        i0 = lax.broadcasted_iota(jnp.int32, (positions, positions), 0)
        i1 = lax.broadcasted_iota(jnp.int32, (positions, positions), 1)
        scale = []
        for i in range(count):
            row = jnp.broadcast_to(keeps[k + i, pl.ds(mine, 1), :], (positions, positions))
            scale.append(jnp.sum(jnp.where(i0 == i1, row, 0.0), axis=1, keepdims=True))
        scale = jnp.concatenate(scale, axis=0)
        log_forget = jnp.log(scale) + jnp.log1p(-loss)
        gate = 1.0 - scale + scale * loss
        j0 = lax.broadcasted_iota(jnp.int32, (size, size), 0)
        j1 = lax.broadcasted_iota(jnp.int32, (size, size), 1)
        later = jnp.where((j1 > j0) & (j0 // positions == j1 // positions), 1.0, 0.0).astype(BF16)
        inside = sum(jnp.dot(later, piece, preferred_element_type=F32) for piece in pieces(log_forget, 3))
        for i in range(count):
            first = i * positions
            logs[pl.ds(peer(k + i), 1), :] = inside[first : first + 1] + log_forget[first : first + 1]
        weighted[pl.ds(k, count)] = (gate * jnp.exp(inside)).reshape(count, positions, width)

    def arrive(k):
        with jax.named_scope("w_direct"):
            direct(k).wait_recv()
        for o in range(1, t):
            forward(k, o, core).start()

    def ready(k):
        with jax.named_scope("w_fwd"):
            keep_copy(k).wait_recv()
            for o in range(1, t):
                forward(k, o, lax.rem(core - o + t, t)).wait_recv()

    arrive(1)
    for j in range(pairs):
        if j < pairs - 1:
            arrive(2 * j + 2)
            arrive(2 * j + 3)
        if j > 0:
            ready(2 * j)
        ready(2 * j + 1)
        with jax.named_scope("forget"):
            forget(2 * j, 2)
        if j < pairs - 1:
            with jax.named_scope("value"):
                value(2 * j, 2)

    def total_copy(o, c):
        return pltpu.make_async_remote_copy(
            src_ref=totals.at[c], dst_ref=totals.at[c],
            send_sem=total_send.at[o], recv_sem=total_recv.at[o],
            device_id=(lax.rem(me + o * members, n), core), device_id_type=MESH,
        )

    def keeper(g):
        return mine * group + g

    def row_copy(g):
        return pltpu.make_async_remote_copy(
            src_ref=totals.at[cube], dst_ref=got_totals.at[cube],
            send_sem=row_send.at[g], recv_sem=row_recv.at[cube],
            device_id=(keeper(g), core), device_id_type=MESH,
        )

    def state_copy(g, b):
        return pltpu.make_async_remote_copy(
            src_ref=states.at[pl.ds(b * batch, batch), pl.ds(g * rows, rows), :],
            dst_ref=got_states.at[cube, pl.ds(b * batch, batch)],
            send_sem=state_send.at[g, b], recv_sem=state_recv.at[cube, b],
            device_id=(keeper(g), core), device_id_type=MESH,
        )

    def read_copy(o, sender):
        return pltpu.make_async_remote_copy(
            src_ref=reads.at[sender], dst_ref=reads.at[sender],
            send_sem=read_send.at[o], recv_sem=read_recv.at[o],
            device_id=(lax.rem(me + o, n), core), device_id_type=MESH,
        )

    def make_states(b):
        for h in range(b * batch, (b + 1) * batch):
            lanes = slice(h * head, (h + 1) * head)
            w = jnp.concatenate([weighted[k, :, lanes] * decays[k : k + 1, lanes] for k in range(members)], axis=0)
            v = values[:, :, lanes].reshape(members * positions, head)
            states[h] = sum(
                lax.dot_general(piece, v, (((0,), (0,)), ((), ())), preferred_element_type=F32)
                for piece in pieces(w, 2)
            )

    def send_states(b):
        for g in range(group):

            @pl.when(keeper(g) != me)
            def _():
                state_copy(g, b).start()

            @pl.when(keeper(g) == me)
            def _():
                got_states[cube, b * batch : (b + 1) * batch] = states[b * batch : (b + 1) * batch, g * rows : (g + 1) * rows, :]

    with jax.named_scope("finish"):
        suffix = jnp.zeros((1, width), F32)
        for p in reversed(range(members)):
            suffixes[p : p + 1, :] = suffix
            suffix = suffix + logs[p : p + 1, :]
        totals[cube] = suffix
        for o in range(1, cubes):
            total_copy(o, cube).start()
        for g in range(group):

            @pl.when(keeper(g) != me)
            def _():
                row_copy(g).start()

            @pl.when(keeper(g) == me)
            def _():
                got_totals[cube] = suffix

        value(members - 2, 2)
        for k in range(members):
            decays[k : k + 1, :] = jnp.exp(suffixes[pl.ds(peer(k), 1), :])
        make_states(0)
        send_states(0)
        for b in range(1, batches):
            make_states(b)
    with jax.named_scope("w_totals"):
        for o in range(1, cubes):
            total_copy(o, lax.rem(cube - o + cubes, cubes)).wait_recv()
    with jax.named_scope("sendreads"):
        later = jnp.zeros((1, width), F32)
        for c in range(cubes):
            later = later + jnp.where(c > cube, totals[c], 0.0)
        decay = jnp.exp(later)
        for h in range(heads):
            lanes = slice(h * head, (h + 1) * head)
            reads[me, :, lanes] = jnp.dot(
                sums[3, :, lanes] * decay[:, lanes], states[h],
                preferred_element_type=F32, precision=lax.Precision.HIGHEST,
            )[0:1]
        for o in range(n - 1, 0, -1):
            read_copy(o, me).start()
        for b in range(1, batches):
            send_states(b)

    source = prompt_of(me // group)
    for c in range(cubes):

        @pl.when(c * members + source != me)
        @jax.named_scope("w_states")
        def _():
            arrivals = [(got_totals.at[c], row_recv.at[c])]
            for b in range(batches):
                arrivals.append((got_states.at[c, pl.ds(b * batch, batch)], state_recv.at[c, b]))
            for piece, arrived in arrivals:
                pltpu.make_async_remote_copy(
                    src_ref=piece, dst_ref=piece,
                    send_sem=row_send.at[0], recv_sem=arrived,
                    device_id=(c * members + source, core), device_id_type=MESH,
                ).wait_recv()

    first = lax.rem(me, group) * rows
    i0 = lax.broadcasted_iota(jnp.int32, (rows, head), 0) + first
    i1 = lax.broadcasted_iota(jnp.int32, (rows, head), 1)
    later = jnp.zeros((1, width), F32)
    final = [got_states[cubes - 1, h] for h in range(heads)]
    for c in reversed(range(cubes - 1)):
        later = later + got_totals[c + 1]
        decay = jnp.exp(later)
        for h in range(heads):
            row = jnp.broadcast_to(decay[:, h * head : (h + 1) * head], (rows, head))
            final[h] = final[h] + got_states[c, h] * jnp.sum(jnp.where(i0 == i1, row, 0.0), axis=1, keepdims=True)
    for h in range(heads):
        cache_out[h] = final[h].astype(BF16)

    with jax.named_scope("w_reads"):
        for o in range(1, n):
            read_copy(o, lax.rem(me - o + n, n)).wait_recv()
    for s in range(s_count):
        row = jnp.zeros((1, width), F32)
        for c in range(cubes):
            row = row + reads[c * members + prompt_of(s)]
        sums[4, s : s + 1, :] = row
    for h in range(heads):
        lanes = slice(h * head, (h + 1) * head)
        mixed = sums[4, :, lanes] + jnp.sum(sums[0, :, lanes], axis=1, keepdims=True) * sums[1, :, lanes]
        normed = mixed * lax.rsqrt(jnp.mean(mixed * mixed, axis=1, keepdims=True) + EPSILON)
        read_out[:, lanes] = (normed * gains[...] * sums[2, :, lanes]).astype(BF16)

    with jax.named_scope("w_sends"):
        for k in range(1, members):
            keep_copy(k).wait_send()
            direct(k).wait_send()
            for o in range(1, t):
                forward(k, o, core).wait_send()
        for o in range(1, t):
            token_copy(o, core).wait_send()
        for o in range(1, cubes):
            total_copy(o, cube).wait_send()
        for g in range(group):

            @pl.when(keeper(g) != me)
            def _():
                row_copy(g).wait_send()
                for b in range(batches):
                    state_copy(g, b).wait_send()

        for o in range(1, n):
            read_copy(o, me).wait_send()


def per_device(prompt, keep_scale, new_token, w_query, w_forget, w_value, w_outgate, floor_gap, norm_gain):
    n, t = lax.axis_size("sp"), lax.axis_size("tp")
    s_count, positions, model = prompt.shape
    head = norm_gain.shape[0]
    width = w_forget.shape[1]
    heads = width // head
    members = s_count
    cubes = n // members
    group = cubes
    rows = head // group
    batches = 2 if heads % 2 == 0 else 1
    sizes = (n, t, s_count, members, cubes, heads, head, rows)
    dma = pltpu.SemaphoreType.DMA
    vmem = pl.BlockSpec(memory_space=pltpu.VMEM)
    hbm = pl.BlockSpec(memory_space=pl.ANY)
    return pl.pallas_call(
        functools.partial(kernel, sizes),
        out_shape=(
            jax.ShapeDtypeStruct((heads, rows, head), BF16),
            jax.ShapeDtypeStruct((s_count, width), BF16),
        ),
        in_specs=[hbm] * 9,
        out_specs=(vmem, vmem),
        scratch_shapes=[
            pltpu.VMEM((members - 1, positions, model // t), BF16),
            pltpu.VMEM((members, positions, model), BF16),
            pltpu.VMEM((members,) + keep_scale.shape, F32),
            pltpu.VMEM((t,) + new_token.shape, BF16),
            pltpu.VMEM((model, width), BF16),
            pltpu.VMEM((model, width), BF16),
            pltpu.VMEM((model, width), BF16),
            pltpu.VMEM((model, width), BF16),
            pltpu.VMEM((1, width), F32),
            pltpu.VMEM((1, head), F32),
            pltpu.VMEM((members, positions, width), F32),
            pltpu.VMEM((members, positions, width), BF16),
            pltpu.VMEM((members, width), F32),
            pltpu.VMEM((members, width), F32),
            pltpu.VMEM((members, width), F32),
            pltpu.VMEM((cubes, 1, width), F32),
            pltpu.VMEM((cubes, 1, width), F32),
            pltpu.VMEM((heads, head, head), F32),
            pltpu.VMEM((cubes, heads, rows, head), F32),
            pltpu.VMEM((n, 1, width), F32),
            pltpu.VMEM((5, s_count, width), F32),
            dma((9,)),
            dma((members,)),
            dma((members,)), dma((members,)),
            dma((members,)), dma((members,)),
            dma((members, t)), dma((members, t)),
            dma((t,)), dma((t,)),
            dma((cubes,)), dma((cubes,)),
            dma((group,)), dma((cubes,)),
            dma((group, batches)), dma((cubes, batches)),
            dma((n,)), dma((n,)),
        ],
        compiler_params=pltpu.CompilerParams(collective_id=0, has_side_effects=True),
    )(
        prompt, keep_scale, new_token, w_query, w_forget, w_value, w_outgate,
        floor_gap.reshape(1, width), norm_gain.reshape(1, head),
    )


def solution(mesh):
    return jax.shard_map(
        per_device,
        mesh=mesh,
        in_specs=(
            P(None, "sp", None),
            P(None, "sp"),
            P(None, "tp"),
            P(None, "tp"),
            P(None, "tp"),
            P(None, "tp"),
            P(None, "tp"),
            P("tp"),
            P(),
        ),
        out_specs=(P("tp", "sp", None), P(None, "tp")),
        check_vma=False,
    )
```

```python
import functools

import jax
import jax.numpy as jnp
from jax import lax
from jax.experimental import pallas as pl
from jax.experimental.pallas import tpu as pltpu
from jax.sharding import PartitionSpec as P

EPSILON = 1e-06
MESH = pl.DeviceIdType.MESH
F32 = jnp.float32
BF16 = jnp.bfloat16


def partner(mine, step, count):
    total, bit = mine, 1
    while bit < count:
        if step // bit % 2:
            total = total + bit * (1 - 2 * lax.rem(mine // bit, 2))
        bit *= 2
    return total


def pieces(x, count):
    out = []
    for _ in range(count):
        piece = x.astype(BF16)
        out.append(piece)
        x = x - piece.astype(F32)
    return out


def arrival_order(members):
    if members == 8:
        return (0, 7, 3, 4, 5, 2, 6, 1)
    return (0,) + tuple(range(members - 1, 0, -1))


def kernel(
    sizes,
    prompt, keep, token, w_query, w_forget, w_value, w_outgate, floor, gain,
    cache_out, read_out,
    stage, blocks, keeps, tokens, wq, wf, wv, wo, floors, gains,
    weighted, values, logs, suffixes, decays, totals, got_totals, states, got_states, reads, sums,
    local_sem, stage_sem, direct_send, direct_recv, keep_send, keep_recv, fwd_send, fwd_recv,
    token_send, token_recv, total_send, total_recv, row_send, row_recv, state_send, state_recv, read_send, read_recv,
):
    n, t, s_count, members, cubes, heads, head, rows = sizes
    group = cubes
    me, core = lax.axis_index("sp"), lax.axis_index("tp")
    cube, place = me // members, lax.rem(me, members)
    model = prompt.shape[2]
    part = model // t
    positions = prompt.shape[1]
    width = heads * head
    order = arrival_order(members)
    pairs = members // 2
    batches = 2 if heads % 2 == 0 else 1
    batch = heads // batches

    def prompt_of(p):
        if members % 4:
            return p
        low = lax.rem(p, 4)
        return p - low + lax.rem(low, 2) * 2 + low // 2

    def columns(c):
        return pl.ds(pl.multiple_of(c * part, part), part)

    peers = [partner(place, r, members) for r in order]

    def peer(k):
        return peers[k]

    mine = prompt_of(place)

    staged = [None] + [
        pltpu.make_async_copy(prompt.at[prompt_of(peer(k)), :, columns(core)], stage.at[k - 1], stage_sem.at[k - 1])
        for k in range(1, members)
    ]
    local = [
        pltpu.make_async_copy(keep, keeps.at[0], local_sem.at[0]),
        pltpu.make_async_copy(token, tokens.at[core], local_sem.at[1]),
        pltpu.make_async_copy(floor, floors, local_sem.at[2]),
        pltpu.make_async_copy(gain, gains, local_sem.at[3]),
        pltpu.make_async_copy(prompt.at[mine], blocks.at[0], local_sem.at[4]),
        pltpu.make_async_copy(w_forget, wf, local_sem.at[5]),
        pltpu.make_async_copy(w_value, wv, local_sem.at[6]),
        pltpu.make_async_copy(w_query, wq, local_sem.at[7]),
        pltpu.make_async_copy(w_outgate, wo, local_sem.at[8]),
    ]

    for k in range(1, members):
        staged[k].start()
    local[0].start()
    local[1].start()
    barrier = pltpu.get_barrier_semaphore()
    for k in range(1, members):
        pl.semaphore_signal(barrier, inc=1, device_id=(cube * members + peer(k), core), device_id_type=MESH)
    for o in range(1, cubes):
        pl.semaphore_signal(barrier, inc=1, device_id=(lax.rem(me + o * members, n), core), device_id_type=MESH)
    for o in range(1, t):
        pl.semaphore_signal(barrier, inc=1, device_id=(me, lax.rem(core + o, t)), device_id_type=MESH)
    for copy in local[2:]:
        copy.start()

    def direct(k):
        return pltpu.make_async_remote_copy(
            src_ref=stage.at[k - 1],
            dst_ref=blocks.at[k, :, columns(core)],
            send_sem=direct_send, recv_sem=direct_recv.at[k - 1],
            device_id=(cube * members + peer(k), core), device_id_type=MESH,
        )

    def keep_copy(k):
        return pltpu.make_async_remote_copy(
            src_ref=keeps.at[0], dst_ref=keeps.at[k],
            send_sem=keep_send, recv_sem=keep_recv,
            device_id=(cube * members + peer(k), core), device_id_type=MESH,
        )

    def forward(k, o, c):
        piece = blocks.at[k, :, columns(c)]
        return pltpu.make_async_remote_copy(
            src_ref=piece, dst_ref=piece,
            send_sem=fwd_send.at[o - 1], recv_sem=fwd_recv.at[k - 1, o - 1],
            device_id=(me, lax.rem(core + o, t)), device_id_type=MESH,
        )

    def token_copy(o, c):
        return pltpu.make_async_remote_copy(
            src_ref=tokens.at[c], dst_ref=tokens.at[c],
            send_sem=token_send.at[o - 1], recv_sem=token_recv.at[o - 1],
            device_id=(me, lax.rem(core + o, t)), device_id_type=MESH,
        )

    local[0].wait()
    local[1].wait()
    with jax.named_scope("barrier"):
        pl.semaphore_wait(barrier, members - 1 + cubes - 1 + t - 1)
    for k in range(1, members):
        keep_copy(k).start()
    for k in range(1, members):
        staged[k].wait()
        direct(k).start()
    for o in range(1, t):
        token_copy(o, core).start()

    with jax.named_scope("wlocal"):
        for copy in local[2:]:
            copy.wait()
        for o in range(1, t):
            token_copy(o, lax.rem(core - o + t, t)).wait_recv()
    floor_row = floors[...]

    with jax.named_scope("token"):
        feature = jnp.concatenate([tokens[c] for c in range(t)], axis=1)
        query = jnp.dot(feature, wq[...], preferred_element_type=F32)
        new_forget = jnp.dot(feature, wf[...], preferred_element_type=F32)
        new_value = jnp.dot(feature, wv[...], preferred_element_type=F32).astype(BF16).astype(F32)
        new_gate = jnp.dot(feature, wo[...], preferred_element_type=F32)
        new_loss = floor_row * (1.0 / (1.0 + jnp.exp(new_forget)))
        read_weight = query * (1.0 - new_loss)
        sums[0] = query * new_loss
        sums[1] = new_value
        sums[2] = new_gate * (1.0 / (1.0 + jnp.exp(-new_gate)))
        seq = lax.broadcasted_iota(jnp.int32, read_weight.shape, 0)
        picked = jnp.where(seq == mine, read_weight, 0.0)
        sums[3] = jnp.broadcast_to(jnp.sum(picked, axis=0, keepdims=True), read_weight.shape)

    def block_rows(k, count):
        return blocks[pl.ds(k, count)].reshape(count * positions, model)

    def value(k, count):
        out = jnp.dot(block_rows(k, count), wv[...], preferred_element_type=F32).astype(BF16)
        values[pl.ds(k, count)] = out.reshape(count, positions, width)

    def forget(k, count):
        size = count * positions
        pre = jnp.dot(block_rows(k, count), wf[...], preferred_element_type=F32)
        loss = floor_row * (1.0 / (1.0 + jnp.exp(pre)))
        i0 = lax.broadcasted_iota(jnp.int32, (positions, positions), 0)
        i1 = lax.broadcasted_iota(jnp.int32, (positions, positions), 1)
        scale = []
        for i in range(count):
            row = jnp.broadcast_to(keeps[k + i, pl.ds(mine, 1), :], (positions, positions))
            scale.append(jnp.sum(jnp.where(i0 == i1, row, 0.0), axis=1, keepdims=True))
        scale = jnp.concatenate(scale, axis=0)
        log_forget = jnp.log(scale * (1.0 - loss))
        gate = 1.0 - scale + scale * loss
        j0 = lax.broadcasted_iota(jnp.int32, (size, size), 0)
        j1 = lax.broadcasted_iota(jnp.int32, (size, size), 1)
        later = jnp.where((j1 > j0) & (j0 // positions == j1 // positions), 1.0, 0.0).astype(BF16)
        inside = sum(jnp.dot(later, piece, preferred_element_type=F32) for piece in pieces(log_forget, 2))
        for i in range(count):
            first = i * positions
            logs[pl.ds(peer(k + i), 1), :] = inside[first : first + 1] + log_forget[first : first + 1]
        weighted[pl.ds(k, count)] = (gate * jnp.exp(inside)).reshape(count, positions, width)

    def arrive(k):
        with jax.named_scope("w_direct"):
            direct(k).wait_recv()
        for o in range(1, t):
            forward(k, o, core).start()

    def ready(k):
        with jax.named_scope("w_fwd"):
            for o in range(1, t):
                forward(k, o, lax.rem(core - o + t, t)).wait_recv()

    def many(ref, send, recv):
        return pltpu.make_async_remote_copy(
            src_ref=ref, dst_ref=ref, send_sem=send, recv_sem=recv,
            device_id=(lax.rem(me + 1, n), core), device_id_type=MESH,
        )

    all_keeps = many(keeps.at[pl.ds(1, members - 1)], keep_send, keep_recv)
    all_direct = many(stage, direct_send, direct_recv.at[0])
    all_totals = many(totals.at[pl.ds(0, cubes - 1)], total_send, total_recv)
    all_reads = many(reads.at[pl.ds(0, n - 1)], read_send, read_recv)

    arrive(1)
    all_keeps.wait_recv()
    for j in range(pairs):
        if j < pairs - 1:
            arrive(2 * j + 2)
            arrive(2 * j + 3)
        if j > 0:
            ready(2 * j)
        ready(2 * j + 1)
        with jax.named_scope("forget"):
            forget(2 * j, 2)
        if j < pairs - 1:
            with jax.named_scope("value"):
                value(2 * j, 2)

    def total_copy(o, c):
        return pltpu.make_async_remote_copy(
            src_ref=totals.at[c], dst_ref=totals.at[c],
            send_sem=total_send, recv_sem=total_recv,
            device_id=(lax.rem(me + o * members, n), core), device_id_type=MESH,
        )

    def keeper(g):
        return mine * group + g

    def row_copy(g):
        return pltpu.make_async_remote_copy(
            src_ref=totals.at[cube], dst_ref=got_totals.at[cube],
            send_sem=row_send.at[g], recv_sem=row_recv.at[cube],
            device_id=(keeper(g), core), device_id_type=MESH,
        )

    def state_copy(g, b):
        return pltpu.make_async_remote_copy(
            src_ref=states.at[pl.ds(b * batch, batch), pl.ds(g * rows, rows), :],
            dst_ref=got_states.at[cube, pl.ds(b * batch, batch)],
            send_sem=state_send.at[g], recv_sem=state_recv.at[cube],
            device_id=(keeper(g), core), device_id_type=MESH,
        )

    def read_copy(o, sender):
        return pltpu.make_async_remote_copy(
            src_ref=reads.at[sender], dst_ref=reads.at[sender],
            send_sem=read_send, recv_sem=read_recv,
            device_id=(lax.rem(me + o, n), core), device_id_type=MESH,
        )

    def make_states(b):
        for h in range(b * batch, (b + 1) * batch):
            lanes = slice(h * head, (h + 1) * head)
            w = jnp.concatenate([weighted[k, :, lanes] * decays[k : k + 1, lanes] for k in range(members)], axis=0)
            v = values[:, :, lanes].reshape(members * positions, head)
            states[h] = sum(
                lax.dot_general(piece, v, (((0,), (0,)), ((), ())), preferred_element_type=F32)
                for piece in pieces(w, 2)
            )

    def send_states(b):
        for g in range(group):

            @pl.when(keeper(g) != me)
            def _():
                state_copy(g, b).start()

            @pl.when(keeper(g) == me)
            def _():
                got_states[cube, b * batch : (b + 1) * batch] = states[b * batch : (b + 1) * batch, g * rows : (g + 1) * rows, :]

    with jax.named_scope("finish"):
        suffix = jnp.zeros((1, width), F32)
        for p in reversed(range(members)):
            suffixes[p : p + 1, :] = suffix
            suffix = suffix + logs[p : p + 1, :]
        totals[cube] = suffix
        for o in range(1, cubes):
            total_copy(o, cube).start()
        for g in range(group):

            @pl.when(keeper(g) != me)
            def _():
                row_copy(g).start()

            @pl.when(keeper(g) == me)
            def _():
                got_totals[cube] = suffix

        value(members - 2, 2)
        for k in range(members):
            decays[k : k + 1, :] = jnp.exp(suffixes[pl.ds(peer(k), 1), :])
        make_states(0)
        send_states(0)
        for b in range(1, batches):
            make_states(b)
    with jax.named_scope("w_totals"):
        all_totals.wait_recv()
    with jax.named_scope("sendreads"):
        later = jnp.zeros((1, width), F32)
        for c in range(cubes):
            later = later + jnp.where(c > cube, totals[c], 0.0)
        decay = jnp.exp(later)
        for h in range(heads):
            lanes = slice(h * head, (h + 1) * head)
            reads[me, :, lanes] = jnp.dot(
                sums[3, :, lanes] * decay[:, lanes], states[h],
                preferred_element_type=F32, precision=lax.Precision.HIGHEST,
            )[0:1]
        for o in range(n - 1, 0, -1):
            read_copy(o, me).start()
        for b in range(1, batches):
            send_states(b)

    source = prompt_of(me // group)
    for c in range(cubes):

        @pl.when(c * members + source != me)
        @jax.named_scope("w_states")
        def _():
            for piece, arrived in ((got_totals.at[c], row_recv.at[c]), (got_states.at[c], state_recv.at[c])):
                pltpu.make_async_remote_copy(
                    src_ref=piece, dst_ref=piece,
                    send_sem=row_send.at[0], recv_sem=arrived,
                    device_id=(c * members + source, core), device_id_type=MESH,
                ).wait_recv()

    first = lax.rem(me, group) * rows
    i0 = lax.broadcasted_iota(jnp.int32, (rows, head), 0) + first
    i1 = lax.broadcasted_iota(jnp.int32, (rows, head), 1)
    later = jnp.zeros((1, width), F32)
    final = [got_states[cubes - 1, h] for h in range(heads)]
    for c in reversed(range(cubes - 1)):
        later = later + got_totals[c + 1]
        decay = jnp.exp(later)
        for h in range(heads):
            row = jnp.broadcast_to(decay[:, h * head : (h + 1) * head], (rows, head))
            final[h] = final[h] + got_states[c, h] * jnp.sum(jnp.where(i0 == i1, row, 0.0), axis=1, keepdims=True)
    for h in range(heads):
        cache_out[h] = final[h].astype(BF16)

    with jax.named_scope("w_reads"):
        all_reads.wait_recv()
    for s in range(s_count):
        row = jnp.zeros((1, width), F32)
        for c in range(cubes):
            row = row + reads[c * members + prompt_of(s)]
        sums[4, s : s + 1, :] = row
    for h in range(heads):
        lanes = slice(h * head, (h + 1) * head)
        mixed = sums[4, :, lanes] + jnp.sum(sums[0, :, lanes], axis=1, keepdims=True) * sums[1, :, lanes]
        normed = mixed * lax.rsqrt(jnp.mean(mixed * mixed, axis=1, keepdims=True) + EPSILON)
        read_out[:, lanes] = (normed * gains[...] * sums[2, :, lanes]).astype(BF16)

    all_keeps.wait_send()
    all_direct.wait_send()
    for o in range(1, t):
        token_copy(o, core).wait_send()
        many(blocks.at[pl.ds(1, members - 1), :, columns(core)], fwd_send.at[o - 1], read_recv).wait_send()
    all_totals.wait_send()
    for g in range(group):

        @pl.when(keeper(g) != me)
        def _():
            row_copy(g).wait_send()
            many(states.at[:, pl.ds(g * rows, rows), :], state_send.at[g], read_recv).wait_send()

    all_reads.wait_send()


def hand_over(cache, read, cache_out, read_out, sem):
    copies = [pltpu.make_async_copy(cache, cache_out, sem.at[0]), pltpu.make_async_copy(read, read_out, sem.at[1])]
    for copy in copies:
        copy.start()
    for copy in copies:
        copy.wait()


def per_device(prompt, keep_scale, new_token, w_query, w_forget, w_value, w_outgate, floor_gap, norm_gain):
    n, t = lax.axis_size("sp"), lax.axis_size("tp")
    s_count, positions, model = prompt.shape
    head = norm_gain.shape[0]
    width = w_forget.shape[1]
    heads = width // head
    members = s_count
    cubes = n // members
    group = cubes
    rows = head // group
    batches = 2 if heads % 2 == 0 else 1
    sizes = (n, t, s_count, members, cubes, heads, head, rows)
    dma = pltpu.SemaphoreType.DMA
    vmem = pl.BlockSpec(memory_space=pltpu.VMEM)
    hbm = pl.BlockSpec(memory_space=pltpu.HBM)
    cache, read = pl.pallas_call(
        functools.partial(kernel, sizes),
        out_shape=(
            pltpu.VMEM((heads, rows, head), BF16),
            pltpu.VMEM((s_count, width), BF16),
        ),
        in_specs=[hbm] * 9,
        out_specs=(vmem, vmem),
        scratch_shapes=[
            pltpu.VMEM((members - 1, positions, model // t), BF16),
            pltpu.VMEM((members, positions, model), BF16),
            pltpu.VMEM((members,) + keep_scale.shape, F32),
            pltpu.VMEM((t,) + new_token.shape, BF16),
            pltpu.VMEM((model, width), BF16),
            pltpu.VMEM((model, width), BF16),
            pltpu.VMEM((model, width), BF16),
            pltpu.VMEM((model, width), BF16),
            pltpu.VMEM((1, width), F32),
            pltpu.VMEM((1, head), F32),
            pltpu.VMEM((members, positions, width), F32),
            pltpu.VMEM((members, positions, width), BF16),
            pltpu.VMEM((members, width), F32),
            pltpu.VMEM((members, width), F32),
            pltpu.VMEM((members, width), F32),
            pltpu.VMEM((cubes, 1, width), F32),
            pltpu.VMEM((cubes, 1, width), F32),
            pltpu.VMEM((heads, head, head), F32),
            pltpu.VMEM((cubes, heads, rows, head), F32),
            pltpu.VMEM((n, 1, width), F32),
            pltpu.VMEM((5, s_count, width), F32),
            dma((9,)), dma((members - 1,)),
            dma, dma((members - 1,)),
            dma, dma,
            dma((t - 1,)), dma((members - 1, t - 1)),
            dma((t - 1,)), dma((t - 1,)),
            dma, dma,
            dma((group,)), dma((cubes,)),
            dma((group,)), dma((cubes,)),
            dma, dma,
        ],
        compiler_params=pltpu.CompilerParams(collective_id=0, has_side_effects=True, vmem_limit_bytes=32*1024*1024),
    )(
        *(
            pltpu.with_memory_space_constraint(x, pltpu.HBM)
            for x in (
                prompt, keep_scale, new_token, w_query, w_forget, w_value, w_outgate,
                floor_gap.reshape(1, width), norm_gain.reshape(1, head),
            )
        )
    )
    return pl.pallas_call(
        hand_over,
        out_shape=(
            jax.ShapeDtypeStruct((heads, rows, head), BF16),
            jax.ShapeDtypeStruct((s_count, width), BF16),
        ),
        in_specs=[vmem, vmem],
        out_specs=(pl.BlockSpec(memory_space=pltpu.HBM), pl.BlockSpec(memory_space=pltpu.HBM)),
        scratch_shapes=[dma((2,))],
        compiler_params=pltpu.CompilerParams(vmem_limit_bytes=1024*1024),
    )(cache, read)


def solution(mesh):
    return jax.shard_map(
        per_device,
        mesh=mesh,
        in_specs=(
            P(None, "sp", None),
            P(None, "sp"),
            P(None, "tp"),
            P(None, "tp"),
            P(None, "tp"),
            P(None, "tp"),
            P(None, "tp"),
            P("tp"),
            P(),
        ),
        out_specs=(P("tp", "sp", None), P(None, "tp")),
        check_vma=False,
    )
```

```python
import functools

import jax
import jax.numpy as jnp
from jax import lax
from jax.experimental import pallas as pl
from jax.experimental.pallas import tpu as pltpu
from jax.sharding import PartitionSpec as P

EPSILON = 1e-06
RANGE = 166.0
TINY = 1e-30
MESH = pl.DeviceIdType.MESH
F32 = jnp.float32
BF16 = jnp.bfloat16


def partner(mine, step, count):
    total, bit = mine, 1
    while bit < count:
        if step // bit % 2:
            total = total + bit * (1 - 2 * lax.rem(mine // bit, 2))
        bit *= 2
    return total


def pieces(x, count):
    out = []
    for _ in range(count):
        piece = x.astype(BF16)
        out.append(piece)
        x = x - piece.astype(F32)
    return out


def arrival_order(members):
    if members == 8:
        return (0, 7, 3, 4, 5, 2, 6, 1)
    return (0,) + tuple(range(members - 1, 0, -1))


def encode(x):
    most = jnp.maximum(jnp.max(jnp.abs(x), axis=0, keepdims=True), TINY)
    level = jnp.exp(RANGE * (jnp.abs(x) * (1.0 / most) - 0.5))
    return jnp.where(x < 0.0, -level, level).astype(BF16), most


def decode(code, most):
    level = code.astype(F32)
    size = (jnp.log(jnp.abs(level)) * (1.0 / RANGE) + 0.5) * most
    return jnp.where(level < 0.0, -size, size)


def kernel(
    sizes,
    prompt, keep, token, w_query, w_forget, w_value, w_outgate, floor, gain,
    cache_out, read_out,
    stage, blocks, keeps, tokens, wq, wf, wv, wo, floors, gains,
    weighted, values, logs, decays, mine_early, early, states, codes, scales, got_codes, got_scales, reads, sums,
    local_sem, stage_sem, other_sem, direct_send, direct_recv, keep_send, keep_recv, fwd_send, fwd_recv,
    token_send, token_recv, early_send, early_recv, scale_send, scale_recv, state_send, state_recv, read_send, read_recv, far_sem,
):
    n, t, s_count, members, cubes, heads, head, rows = sizes
    group = cubes
    me, core = lax.axis_index("sp"), lax.axis_index("tp")
    cube, place = me // members, lax.rem(me, members)
    model = prompt.shape[2]
    part = model // t
    positions = prompt.shape[1]
    width = heads * head
    order = arrival_order(members)
    pairs = members // 2
    batches = 2 if heads % 2 == 0 else 1
    batch = heads // batches

    def prompt_of(p):
        if members % 4:
            return p
        low = lax.rem(p, 4)
        return p - low + lax.rem(low, 2) * 2 + low // 2

    def columns(c):
        return pl.ds(pl.multiple_of(c * part, part), part)

    peers = [partner(place, r, members) for r in order]
    prompts = [prompt_of(p) for p in peers]
    mine = prompts[0]

    def staging(k, c, sem):
        return pltpu.make_async_copy(prompt.at[prompts[k], :, columns(c)], stage.at[k, :, columns(c)], sem)

    staged = [staging(k, core, stage_sem.at[k]) for k in range(members)]
    others = [lax.rem(core + o, t) for o in range(1, t)]
    local = [
        pltpu.make_async_copy(keep, keeps.at[0], local_sem.at[0]),
        pltpu.make_async_copy(token, tokens.at[core], local_sem.at[1]),
        pltpu.make_async_copy(floor, floors, local_sem.at[2]),
        pltpu.make_async_copy(gain, gains, local_sem.at[3]),
        pltpu.make_async_copy(prompt.at[mine], blocks.at[0], local_sem.at[4]),
        pltpu.make_async_copy(w_forget, wf, local_sem.at[5]),
        pltpu.make_async_copy(w_value, wv, local_sem.at[6]),
        pltpu.make_async_copy(w_query, wq, local_sem.at[7]),
        pltpu.make_async_copy(w_outgate, wo, local_sem.at[8]),
    ]

    staged[1].start()
    local[0].start()
    local[1].start()
    barrier = pltpu.get_barrier_semaphore()
    for k in range(1, members):
        pl.semaphore_signal(barrier, inc=1, device_id=(cube * members + peers[k], core), device_id_type=MESH)
    for o in range(1, cubes):
        pl.semaphore_signal(barrier, inc=1, device_id=(lax.rem(me + o * members, n), core), device_id_type=MESH)
    for o in range(1, t):
        pl.semaphore_signal(barrier, inc=1, device_id=(me, lax.rem(core + o, t)), device_id_type=MESH)
    for k in range(2, members):
        staged[k].start()
    staged[0].start()

    def direct(k):
        return pltpu.make_async_remote_copy(
            src_ref=stage.at[k, :, columns(core)],
            dst_ref=blocks.at[k, :, columns(core)],
            send_sem=direct_send, recv_sem=direct_recv.at[k - 1],
            device_id=(cube * members + peers[k], core), device_id_type=MESH,
        )

    def keep_copy(k):
        return pltpu.make_async_remote_copy(
            src_ref=keeps.at[0], dst_ref=keeps.at[k],
            send_sem=keep_send, recv_sem=keep_recv,
            device_id=(cube * members + peers[k], core), device_id_type=MESH,
        )

    def forward(k, o, c):
        piece = blocks.at[k, :, columns(c)]
        return pltpu.make_async_remote_copy(
            src_ref=piece, dst_ref=piece,
            send_sem=fwd_send.at[o - 1], recv_sem=fwd_recv.at[k - 1, o - 1],
            device_id=(me, lax.rem(core + o, t)), device_id_type=MESH,
        )

    def token_copy(o, c):
        return pltpu.make_async_remote_copy(
            src_ref=tokens.at[c], dst_ref=tokens.at[c],
            send_sem=token_send.at[o - 1], recv_sem=token_recv.at[o - 1],
            device_id=(me, lax.rem(core + o, t)), device_id_type=MESH,
        )

    def early_copy(o, k):
        return pltpu.make_async_remote_copy(
            src_ref=mine_early.at[k], dst_ref=early.at[me],
            send_sem=early_send, recv_sem=early_recv,
            device_id=(lax.rem(cube + o, cubes) * members + peers[k], core), device_id_type=MESH,
        )

    def keeper(g):
        return mine * group + g

    def scale_copy(g):
        return pltpu.make_async_remote_copy(
            src_ref=scales.at[g], dst_ref=got_scales.at[cube],
            send_sem=scale_send.at[g], recv_sem=scale_recv.at[cube],
            device_id=(keeper(g), core), device_id_type=MESH,
        )

    def state_copy(g, b):
        return pltpu.make_async_remote_copy(
            src_ref=codes.at[pl.ds(b * batch, batch), pl.ds(g * rows, rows), :],
            dst_ref=got_codes.at[cube, pl.ds(b * batch, batch)],
            send_sem=state_send.at[g], recv_sem=state_recv.at[cube],
            device_id=(keeper(g), core), device_id_type=MESH,
        )

    def read_copy(o, sender):
        return pltpu.make_async_remote_copy(
            src_ref=reads.at[sender], dst_ref=reads.at[sender],
            send_sem=read_send, recv_sem=read_recv,
            device_id=(lax.rem(me + o, n), core), device_id_type=MESH,
        )

    def many(ref, send, recv):
        return pltpu.make_async_remote_copy(
            src_ref=ref, dst_ref=ref, send_sem=send, recv_sem=recv,
            device_id=(lax.rem(me + 1, n), core), device_id_type=MESH,
        )

    all_keeps = many(keeps.at[pl.ds(1, members - 1)], keep_send, keep_recv)
    all_direct = many(blocks.at[pl.ds(1, members - 1), :, columns(core)], direct_send, direct_recv.at[0])
    all_early = many(early.at[pl.ds(0, n - members)], early_send, early_recv)
    all_reads = many(reads.at[pl.ds(0, n - 1)], read_send, read_recv)

    local[0].wait()
    local[1].wait()
    with jax.named_scope("barrier"):
        pl.semaphore_wait(barrier, members - 1 + cubes - 1 + t - 1)
    for k in range(1, members):
        pl.semaphore_signal(far_sem, inc=1, device_id=(cube * members + peers[k], core), device_id_type=MESH)
        keep_copy(k).start()
    for k in range(1, members):
        staged[k].wait()
        direct(k).start()
    for o in range(1, t):
        token_copy(o, core).start()
    for i, c in enumerate(others):
        for k in range(members):
            staging(k, c, other_sem.at[i]).start()
    for i in (2, 5, 6, 7, 8, 4, 3):
        local[i].start()

    with jax.named_scope("wlocal"):
        staged[0].wait()
        for i, c in enumerate(others):
            half = stage.at[:, :, columns(c)]
            pltpu.make_async_copy(half, half, other_sem.at[i]).wait()
        local[2].wait()
        local[5].wait()
    floor_row = floors[...]
    p0 = lax.broadcasted_iota(jnp.int32, (positions, positions), 0)
    p1 = lax.broadcasted_iota(jnp.int32, (positions, positions), 1)

    def column(row):
        return jnp.sum(jnp.where(p0 == p1, jnp.broadcast_to(row, (positions, positions)), 0.0), axis=1, keepdims=True)

    def losses(x, lanes):
        pre = jnp.dot(x, wf[:, lanes], preferred_element_type=F32)
        return floor_row[:, lanes] * (1.0 / (1.0 + jnp.exp(pre)))

    every = slice(0, width)
    with jax.named_scope("early"):
        half = members // 2
        for k in range(0, members, half):
            x = stage[k : k + half].reshape(half * positions, model)
            scale = jnp.concatenate([column(keeps[0, pl.ds(prompts[k + i], 1), :]) for i in range(half)], axis=0)
            log_forget = jnp.log(scale * (1.0 - losses(x, every))).reshape(half, positions, width)
            mine_early[k : k + half] = jnp.sum(log_forget, axis=1, keepdims=True)
        pl.semaphore_wait(far_sem, members - 1)
        for o in range(1, cubes):
            for k in range(members):
                early_copy(o, k).start()
        early[pl.ds(cube * members, members)] = jnp.zeros((members, 1, width), F32)

    with jax.named_scope("wlocal2"):
        for i in (6, 7, 8, 4, 3):
            local[i].wait()
        for o in range(1, t):
            token_copy(o, lax.rem(core - o + t, t)).wait_recv()
    with jax.named_scope("token"):
        feature = jnp.concatenate([tokens[c] for c in range(t)], axis=1)
        query = jnp.dot(feature, wq[...], preferred_element_type=F32)
        new_forget = jnp.dot(feature, wf[...], preferred_element_type=F32)
        new_value = jnp.dot(feature, wv[...], preferred_element_type=F32).astype(BF16).astype(F32)
        new_gate = jnp.dot(feature, wo[...], preferred_element_type=F32)
        new_loss = floor_row * (1.0 / (1.0 + jnp.exp(new_forget)))
        read_weight = query * (1.0 - new_loss)
        sums[0] = query * new_loss
        sums[1] = new_value
        sums[2] = new_gate * (1.0 / (1.0 + jnp.exp(-new_gate)))
        seq = lax.broadcasted_iota(jnp.int32, read_weight.shape, 0)
        picked = jnp.where(seq == mine, read_weight, 0.0)
        sums[3] = jnp.broadcast_to(jnp.sum(picked, axis=0, keepdims=True), read_weight.shape)

    def block_rows(k, count):
        return blocks[k : k + count].reshape(count * positions, model)

    def value(k, count, lanes):
        out = jnp.dot(block_rows(k, count), wv[:, lanes], preferred_element_type=F32).astype(BF16)
        values[k : k + count, :, lanes] = out.reshape(count, positions, -1)

    def forget(k, count, lanes):
        size = count * positions
        loss = losses(block_rows(k, count), lanes)
        scale = jnp.concatenate([column(keeps[k + i, pl.ds(mine, 1), :]) for i in range(count)], axis=0)
        log_forget = jnp.log(scale * (1.0 - loss))
        gate = 1.0 - scale + scale * loss
        j0 = lax.broadcasted_iota(jnp.int32, (size, size), 0)
        j1 = lax.broadcasted_iota(jnp.int32, (size, size), 1)
        later = jnp.where((j1 > j0) & (j0 // positions == j1 // positions), 1.0, 0.0).astype(BF16)
        inside = sum(jnp.dot(later, piece, preferred_element_type=F32) for piece in pieces(log_forget, 2))
        for i in range(count):
            first = i * positions
            logs[peers[k + i], :, lanes] = inside[first : first + 1] + log_forget[first : first + 1]
        weighted[k : k + count, :, lanes] = (gate * jnp.exp(inside)).reshape(count, positions, -1)

    def arrive(k):
        with jax.named_scope("w_direct"):
            direct(k).wait_recv()
        for o in range(1, t):
            forward(k, o, core).start()

    def ready(k):
        with jax.named_scope("w_fwd"):
            for o in range(1, t):
                forward(k, o, lax.rem(core - o + t, t)).wait_recv()

    arrive(1)
    all_keeps.wait_recv()
    for j in range(pairs):
        if j < pairs - 1:
            arrive(2 * j + 2)
            arrive(2 * j + 3)
        if j > 0:
            ready(2 * j)
        ready(2 * j + 1)
        if j < pairs - 1:
            with jax.named_scope("forget"):
                forget(2 * j, 2, every)
            with jax.named_scope("value"):
                value(2 * j, 2, every)

    with jax.named_scope("w_early"):
        all_early.wait_recv()
    after = jnp.zeros((1, width), F32)
    for c in range(1, cubes):
        block = early[c * members]
        for p in range(1, members):
            block = block + early[c * members + p]
        after = after + jnp.where(c > cube, block, 0.0)

    with jax.named_scope("tail_forget"):
        forget(members - 2, 2, every)
        value(members - 2, 2, every)
        suffix = after
        for p in reversed(range(members)):
            decays[p] = jnp.exp(suffix)
            suffix = suffix + logs[p]
    for b in range(batches):
        with jax.named_scope("tail_states"):
            for h in range(b * batch, (b + 1) * batch):
                own = slice(h * head, (h + 1) * head)
                w = jnp.concatenate(
                    [weighted[k, :, own] * decays[peers[k], :, own] for k in range(members)], axis=0
                )
                v = values[:, :, own].reshape(members * positions, head)
                states[h] = sum(
                    lax.dot_general(piece, v, (((0,), (0,)), ((), ())), preferred_element_type=F32)
                    for piece in pieces(w, 2)
                )
        if b == batches - 1:
            with jax.named_scope("sendreads"):
                for h in range(heads):
                    own = slice(h * head, (h + 1) * head)
                    reads[me, :, own] = jnp.dot(
                        sums[3, :, own], states[h], preferred_element_type=F32, precision=lax.Precision.HIGHEST
                    )[0:1]
                for o in range(n - 1, 0, -1):
                    read_copy(o, me).start()
        with jax.named_scope("tail_codes"):
            for h in range(b * batch, (b + 1) * batch):
                own = slice(h * head, (h + 1) * head)
                for g in range(group):
                    span = slice(g * rows, (g + 1) * rows)
                    codes[h, span], scales[g, :, own] = encode(states[h, span])
            for g in range(group):

                @pl.when(keeper(g) != me)
                def _():
                    if b == batches - 1:
                        scale_copy(g).start()
                    state_copy(g, b).start()

                @pl.when(keeper(g) == me)
                def _():
                    span = slice(g * rows, (g + 1) * rows)
                    got_codes[cube, b * batch : (b + 1) * batch] = codes[b * batch : (b + 1) * batch, span]
                    if b == batches - 1:
                        got_scales[cube] = scales[g]

    source = prompt_of(me // group)
    for c in range(cubes):

        @pl.when(c * members + source != me)
        @jax.named_scope("w_states")
        def _():
            for piece, arrived in ((got_scales.at[c], scale_recv.at[c]), (got_codes.at[c], state_recv.at[c])):
                pltpu.make_async_remote_copy(
                    src_ref=piece, dst_ref=piece,
                    send_sem=read_send, recv_sem=arrived,
                    device_id=(c * members + source, core), device_id_type=MESH,
                ).wait_recv()

    for h in range(heads):
        own = slice(h * head, (h + 1) * head)
        cache_out[h] = sum(decode(got_codes[c, h], got_scales[c, :, own]) for c in range(cubes)).astype(BF16)

    with jax.named_scope("w_reads"):
        all_reads.wait_recv()
    for s in range(s_count):
        row = jnp.zeros((1, width), F32)
        for c in range(cubes):
            row = row + reads[c * members + prompt_of(s)]
        sums[4, s : s + 1, :] = row
    for h in range(heads):
        lanes = slice(h * head, (h + 1) * head)
        mixed = sums[4, :, lanes] + jnp.sum(sums[0, :, lanes], axis=1, keepdims=True) * sums[1, :, lanes]
        normed = mixed * lax.rsqrt(jnp.mean(mixed * mixed, axis=1, keepdims=True) + EPSILON)
        read_out[:, lanes] = (normed * gains[...] * sums[2, :, lanes]).astype(BF16)

    all_keeps.wait_send()
    all_direct.wait_send()
    for o in range(1, t):
        token_copy(o, core).wait_send()
        many(blocks.at[pl.ds(1, members - 1), :, columns(core)], fwd_send.at[o - 1], read_recv).wait_send()
    all_early.wait_send()
    for g in range(group):

        @pl.when(keeper(g) != me)
        def _():
            scale_copy(g).wait_send()
            many(codes.at[:, pl.ds(g * rows, rows), :], state_send.at[g], read_recv).wait_send()

    all_reads.wait_send()


def hand_over(cache, read, cache_out, read_out, sem):
    copies = [pltpu.make_async_copy(cache, cache_out, sem.at[0]), pltpu.make_async_copy(read, read_out, sem.at[1])]
    for copy in copies:
        copy.start()
    for copy in copies:
        copy.wait()


def per_device(prompt, keep_scale, new_token, w_query, w_forget, w_value, w_outgate, floor_gap, norm_gain):
    n, t = lax.axis_size("sp"), lax.axis_size("tp")
    s_count, positions, model = prompt.shape
    head = norm_gain.shape[0]
    width = w_forget.shape[1]
    heads = width // head
    members = s_count
    cubes = n // members
    group = cubes
    rows = head // group
    batches = 2 if heads % 2 == 0 else 1
    sizes = (n, t, s_count, members, cubes, heads, head, rows)
    dma = pltpu.SemaphoreType.DMA
    vmem = pl.BlockSpec(memory_space=pltpu.VMEM)
    hbm = pl.BlockSpec(memory_space=pltpu.HBM)
    cache, read = pl.pallas_call(
        functools.partial(kernel, sizes),
        out_shape=(
            pltpu.VMEM((heads, rows, head), BF16),
            pltpu.VMEM((s_count, width), BF16),
        ),
        in_specs=[hbm] * 9,
        out_specs=(vmem, vmem),
        scratch_shapes=[
            pltpu.VMEM((members, positions, model), BF16),
            pltpu.VMEM((members, positions, model), BF16),
            pltpu.VMEM((members,) + keep_scale.shape, F32),
            pltpu.VMEM((t,) + new_token.shape, BF16),
            pltpu.VMEM((model, width), BF16),
            pltpu.VMEM((model, width), BF16),
            pltpu.VMEM((model, width), BF16),
            pltpu.VMEM((model, width), BF16),
            pltpu.VMEM((1, width), F32),
            pltpu.VMEM((1, head), F32),
            pltpu.VMEM((members, positions, width), F32),
            pltpu.VMEM((members, positions, width), BF16),
            pltpu.VMEM((members, 1, width), F32),
            pltpu.VMEM((members, 1, width), F32),
            pltpu.VMEM((members, 1, width), F32),
            pltpu.VMEM((n, 1, width), F32),
            pltpu.VMEM((heads, head, head), F32),
            pltpu.VMEM((heads, head, head), BF16),
            pltpu.VMEM((group, 1, width), F32),
            pltpu.VMEM((cubes, heads, rows, head), BF16),
            pltpu.VMEM((cubes, 1, width), F32),
            pltpu.VMEM((n, 1, width), F32),
            pltpu.VMEM((5, s_count, width), F32),
            dma((9,)), dma((members,)), dma((t - 1,)),
            dma, dma((members - 1,)),
            dma, dma,
            dma((t - 1,)), dma((members - 1, t - 1)),
            dma((t - 1,)), dma((t - 1,)),
            dma, dma,
            dma((group,)), dma((cubes,)),
            dma((group,)), dma((cubes,)),
            dma, dma,
            pltpu.SemaphoreType.REGULAR,
        ],
        compiler_params=pltpu.CompilerParams(collective_id=0, has_side_effects=True, vmem_limit_bytes=32*1024*1024),
    )(
        *(
            pltpu.with_memory_space_constraint(x, pltpu.HBM)
            for x in (
                prompt, keep_scale, new_token, w_query, w_forget, w_value, w_outgate,
                floor_gap.reshape(1, width), norm_gain.reshape(1, head),
            )
        )
    )
    return pl.pallas_call(
        hand_over,
        out_shape=(
            jax.ShapeDtypeStruct((heads, rows, head), BF16),
            jax.ShapeDtypeStruct((s_count, width), BF16),
        ),
        in_specs=[vmem, vmem],
        out_specs=(pl.BlockSpec(memory_space=pltpu.HBM), pl.BlockSpec(memory_space=pltpu.HBM)),
        scratch_shapes=[dma((2,))],
        compiler_params=pltpu.CompilerParams(vmem_limit_bytes=1024*1024),
    )(cache, read)


def solution(mesh):
    return jax.shard_map(
        per_device,
        mesh=mesh,
        in_specs=(
            P(None, "sp", None),
            P(None, "sp"),
            P(None, "tp"),
            P(None, "tp"),
            P(None, "tp"),
            P(None, "tp"),
            P(None, "tp"),
            P("tp"),
            P(),
        ),
        out_specs=(P("tp", "sp", None), P(None, "tp")),
        check_vma=False,
    )
```

```python
import functools

import jax
import jax.numpy as jnp
from jax import lax
from jax.experimental import pallas as pl
from jax.experimental.pallas import tpu as pltpu
from jax.sharding import PartitionSpec as P

EPSILON = 1e-06
RANGE = 166.0
TINY = 1e-30
MESH = pl.DeviceIdType.MESH
F32 = jnp.float32
BF16 = jnp.bfloat16


def partner(mine, step, count):
    total, bit = mine, 1
    while bit < count:
        if step // bit % 2:
            total = total + bit * (1 - 2 * lax.rem(mine // bit, 2))
        bit *= 2
    return total


def pieces(x, count):
    out = []
    for _ in range(count):
        piece = x.astype(BF16)
        out.append(piece)
        x = x - piece.astype(F32)
    return out


def arrival_order(members):
    if members == 8:
        return (0, 7, 3, 4, 5, 2, 6, 1)
    return (0,) + tuple(range(members - 1, 0, -1))


def encode(x):
    most = jnp.maximum(jnp.max(jnp.abs(x), axis=0, keepdims=True), TINY)
    level = jnp.exp(RANGE * (jnp.abs(x) * (1.0 / most) - 0.5))
    return jnp.where(x < 0.0, -level, level).astype(BF16), most


def decode(code, most):
    level = code.astype(F32)
    size = (jnp.log(jnp.abs(level)) * (1.0 / RANGE) + 0.5) * most
    return jnp.where(level < 0.0, -size, size)


def kernel(
    sizes,
    prompt, keep, token, w_query, w_forget, w_value, w_outgate, floor, gain,
    cache_out, read_out,
    stage, blocks, keeps, rows_in, tokens, wf, weights, floors, gains,
    weighted, values, logs, decays, mine_early, early, states, codes, scales, got_codes, got_scales, reads, sums, query_down,
    local_sem, stage_sem, other_sem, direct_send, direct_recv, keep_send, keep_recv, fwd_send, fwd_recv,
    token_send, token_recv, early_send, early_recv, scale_send, scale_recv, state_send, state_recv, read_send, read_recv, far_sem,
):
    n, t, s_count, members, cubes, heads, head, rows = sizes
    group = cubes
    me, core = lax.axis_index("sp"), lax.axis_index("tp")
    cube, place = me // members, lax.rem(me, members)
    model = prompt.shape[2]
    part = model // t
    positions = prompt.shape[1]
    width = heads * head
    order = arrival_order(members)
    pairs = members // 2

    def prompt_of(p):
        if members % 4:
            return p
        low = lax.rem(p, 4)
        return p - low + lax.rem(low, 2) * 2 + low // 2

    def columns(c):
        return pl.ds(pl.multiple_of(c * part, part), part)

    peers = [partner(place, r, members) for r in order]
    prompts = [prompt_of(p) for p in peers]
    mine = prompts[0]

    def staging(k, c, sem):
        return pltpu.make_async_copy(prompt.at[prompts[k], :, columns(c)], stage.at[k, :, columns(c)], sem)

    staged = [staging(k, core, stage_sem.at[1 if k == 1 else 0]) for k in range(members)]
    others = [lax.rem(core + o, t) for o in range(1, t)]
    local = [
        pltpu.make_async_copy(keep, keeps.at[0], local_sem.at[0]),
        pltpu.make_async_copy(token, tokens.at[core], local_sem.at[1]),
        pltpu.make_async_copy(floor, floors, local_sem.at[2]),
        pltpu.make_async_copy(gain, gains, local_sem.at[3]),
        pltpu.make_async_copy(prompt.at[mine], blocks.at[0], local_sem.at[4]),
        pltpu.make_async_copy(w_forget, wf, local_sem.at[5]),
        pltpu.make_async_copy(w_value, weights.at[0], local_sem.at[6]),
        pltpu.make_async_copy(w_query, weights.at[1], local_sem.at[6]),
        pltpu.make_async_copy(w_outgate, weights.at[2], local_sem.at[6]),
    ]

    staged[1].start()
    local[0].start()
    local[1].start()
    barrier = pltpu.get_barrier_semaphore()
    for k in range(1, members):
        pl.semaphore_signal(barrier, inc=1, device_id=(cube * members + peers[k], core), device_id_type=MESH)
    for o in range(1, cubes):
        pl.semaphore_signal(barrier, inc=1, device_id=(lax.rem(me + o * members, n), core), device_id_type=MESH)
    for o in range(1, t):
        pl.semaphore_signal(barrier, inc=1, device_id=(me, lax.rem(core + o, t)), device_id_type=MESH)
    for k in range(2, members):
        staged[k].start()
    staged[0].start()

    def direct(k):
        return pltpu.make_async_remote_copy(
            src_ref=stage.at[k, :, columns(core)],
            dst_ref=blocks.at[k, :, columns(core)],
            send_sem=direct_send, recv_sem=direct_recv.at[k // 2],
            device_id=(cube * members + peers[k], core), device_id_type=MESH,
        )

    def keep_copy(k):
        return pltpu.make_async_remote_copy(
            src_ref=keeps.at[0, pl.ds(prompts[k], 1)], dst_ref=rows_in.at[k - 1],
            send_sem=keep_send, recv_sem=keep_recv,
            device_id=(cube * members + peers[k], core), device_id_type=MESH,
        )

    def landed(j, c):
        return blocks.at[pl.ds(max(2 * j, 1), 2 if j else 1), :, columns(c)]

    def forward(j, o, c):
        piece = landed(j, c)
        return pltpu.make_async_remote_copy(
            src_ref=piece, dst_ref=piece,
            send_sem=fwd_send.at[o - 1], recv_sem=fwd_recv.at[j, o - 1],
            device_id=(me, lax.rem(core + o, t)), device_id_type=MESH,
        )

    def token_copy(o, c):
        return pltpu.make_async_remote_copy(
            src_ref=tokens.at[c], dst_ref=tokens.at[c],
            send_sem=token_send.at[o - 1], recv_sem=token_recv.at[o - 1],
            device_id=(me, lax.rem(core + o, t)), device_id_type=MESH,
        )

    def early_copy(o, k):
        return pltpu.make_async_remote_copy(
            src_ref=mine_early.at[k], dst_ref=early.at[me],
            send_sem=early_send, recv_sem=early_recv,
            device_id=(lax.rem(cube + o, cubes) * members + peers[k], core), device_id_type=MESH,
        )

    def keeper(g):
        return mine * group + g

    def scale_copy(g):
        return pltpu.make_async_remote_copy(
            src_ref=scales.at[g], dst_ref=got_scales.at[cube],
            send_sem=scale_send.at[g], recv_sem=scale_recv.at[cube],
            device_id=(keeper(g), core), device_id_type=MESH,
        )

    def state_copy(g):
        return pltpu.make_async_remote_copy(
            src_ref=codes.at[:, pl.ds(g * rows, rows), :],
            dst_ref=got_codes.at[cube],
            send_sem=state_send.at[g], recv_sem=state_recv.at[cube],
            device_id=(keeper(g), core), device_id_type=MESH,
        )

    def read_copy(o, sender):
        return pltpu.make_async_remote_copy(
            src_ref=reads.at[sender], dst_ref=reads.at[sender],
            send_sem=read_send, recv_sem=read_recv,
            device_id=(lax.rem(me + o, n), core), device_id_type=MESH,
        )

    def many(ref, send, recv):
        return pltpu.make_async_remote_copy(
            src_ref=ref, dst_ref=ref, send_sem=send, recv_sem=recv,
            device_id=(lax.rem(me + 1, n), core), device_id_type=MESH,
        )

    all_keeps = many(rows_in, keep_send, keep_recv)
    all_direct = many(blocks.at[pl.ds(1, members - 1), :, columns(core)], direct_send, direct_recv.at[0])
    all_early = many(early.at[pl.ds(0, n - members)], early_send, early_recv)
    all_reads = many(reads.at[pl.ds(0, n - 1)], read_send, read_recv)

    with jax.named_scope("barrier"):
        pl.semaphore_wait(barrier, members - 1 + cubes - 1 + t - 1)
    staged[1].wait()
    direct(1).start()
    rest = stage.at[pl.ds(1, members - 1), :, columns(core)]
    pltpu.make_async_copy(rest, rest, stage_sem.at[0]).wait()
    for k in range(2, members):
        direct(k).start()
        if k == members // 2 - 1:
            local[0].wait()
            for i in range(1, members):
                keep_copy(i).start()
    for k in range(1, members):
        pl.semaphore_signal(far_sem, inc=1, device_id=(cube * members + peers[k], core), device_id_type=MESH)
    local[1].wait()
    for o in range(1, t):
        token_copy(o, core).start()
    for i, c in enumerate(others):
        for k in range(members):
            staging(k, c, other_sem.at[i]).start()
    for i in (2, 5, 6, 7, 8, 4, 3):
        local[i].start()

    with jax.named_scope("wlocal"):
        for i, c in enumerate(others):
            half = stage.at[:, :, columns(c)]
            pltpu.make_async_copy(half, half, other_sem.at[i]).wait()
        local[2].wait()
        local[5].wait()
    floor_row = floors[...]
    p0 = lax.broadcasted_iota(jnp.int32, (positions, positions), 0)
    p1 = lax.broadcasted_iota(jnp.int32, (positions, positions), 1)

    def column(row):
        return jnp.sum(jnp.where(p0 == p1, jnp.broadcast_to(row, (positions, positions)), 0.0), axis=1, keepdims=True)

    def losses(x, lanes):
        pre = jnp.dot(x, wf[:, lanes], preferred_element_type=F32)
        return floor_row[:, lanes] * (1.0 / (1.0 + jnp.exp(pre)))

    every = slice(0, width)
    with jax.named_scope("early"):
        half = members // 2
        for k in range(0, members, half):
            x = stage[k : k + half].reshape(half * positions, model)
            scale = jnp.concatenate([column(keeps[0, pl.ds(prompts[k + i], 1), :]) for i in range(half)], axis=0)
            log_forget = jnp.log(scale * (1.0 - losses(x, every))).reshape(half, positions, width)
            mine_early[k : k + half] = jnp.sum(log_forget, axis=1, keepdims=True)
        pl.semaphore_wait(far_sem, members - 1)
        for o in range(1, cubes):
            for k in range(members):
                early_copy(o, k).start()
        early[pl.ds(cube * members, members)] = jnp.zeros((members, 1, width), F32)

    with jax.named_scope("wlocal2"):
        pltpu.make_async_copy(weights, weights, local_sem.at[6]).wait()
        local[4].wait()
        local[3].wait()
        for o in range(1, t):
            token_copy(o, lax.rem(core - o + t, t)).wait_recv()
    with jax.named_scope("token"):
        feature = jnp.concatenate([tokens[c] for c in range(t)], axis=1)
        query = jnp.dot(feature, weights[1], preferred_element_type=F32)
        new_forget = jnp.dot(feature, wf[...], preferred_element_type=F32)
        new_value = jnp.dot(feature, weights[0], preferred_element_type=F32).astype(BF16).astype(F32)
        new_gate = jnp.dot(feature, weights[2], preferred_element_type=F32)
        new_loss = floor_row * (1.0 / (1.0 + jnp.exp(new_forget)))
        read_weight = query * (1.0 - new_loss)
        sums[0] = query * new_loss
        sums[1] = new_value
        sums[2] = new_gate * (1.0 / (1.0 + jnp.exp(-new_gate)))
        seq = lax.broadcasted_iota(jnp.int32, read_weight.shape, 0)
        picked = jnp.where(seq == mine, read_weight, 0.0)
        weight = jnp.sum(picked, axis=0, keepdims=True)
        h0 = lax.broadcasted_iota(jnp.int32, (head, head), 0)
        h1 = lax.broadcasted_iota(jnp.int32, (head, head), 1)
        for h in range(heads):
            row = jnp.broadcast_to(weight[:, h * head : (h + 1) * head], (head, head))
            down = jnp.sum(jnp.where(h0 == h1, row, 0.0), axis=1, keepdims=True)
            query_down[h] = jnp.broadcast_to(down, (head, head))

    def block_rows(k, count):
        return blocks[k : k + count].reshape(count * positions, model)

    def value(k, count, lanes):
        out = jnp.dot(block_rows(k, count), weights[0, :, lanes], preferred_element_type=F32).astype(BF16)
        values[k : k + count, :, lanes] = out.reshape(count, positions, -1)

    def forget(k, count, lanes):
        size = count * positions
        loss = losses(block_rows(k, count), lanes)
        scale = jnp.concatenate([column(rows_in[k + i - 1] if k + i else keeps[0, pl.ds(mine, 1), :]) for i in range(count)], axis=0)
        log_forget = jnp.log(scale * (1.0 - loss))
        gate = 1.0 - scale + scale * loss
        j0 = lax.broadcasted_iota(jnp.int32, (size, size), 0)
        j1 = lax.broadcasted_iota(jnp.int32, (size, size), 1)
        later = jnp.where((j1 > j0) & (j0 // positions == j1 // positions), 1.0, 0.0).astype(BF16)
        inside = sum(jnp.dot(later, piece, preferred_element_type=F32) for piece in pieces(log_forget, 2))
        for i in range(count):
            first = i * positions
            logs[peers[k + i], :, lanes] = inside[first : first + 1] + log_forget[first : first + 1]
        weighted[k : k + count, :, lanes] = (gate * jnp.exp(inside)).reshape(count, positions, -1)

    def arrive(j):
        with jax.named_scope("w_direct"):
            many(landed(j, core), direct_send, direct_recv.at[j]).wait_recv()
        for o in range(1, t):
            forward(j, o, core).start()

    arrive(0)
    all_keeps.wait_recv()
    for j in range(pairs):
        if j < pairs - 1:
            arrive(j + 1)
        with jax.named_scope("w_fwd"):
            for o in range(1, t):
                forward(j, o, lax.rem(core - o + t, t)).wait_recv()
        if j < pairs - 1:
            with jax.named_scope("pair"):
                forget(2 * j, 2, every)
                value(2 * j, 2, every)

    with jax.named_scope("w_early"):
        all_early.wait_recv()
    after = jnp.zeros((1, width), F32)
    for c in range(1, cubes):
        block = early[c * members]
        for p in range(1, members):
            block = block + early[c * members + p]
        after = after + jnp.where(c > cube, block, 0.0)

    with jax.named_scope("tail_forget"):
        forget(members - 2, 2, every)
        value(members - 2, 2, every)
        suffix = after
        for p in reversed(range(members)):
            decays[p] = jnp.exp(suffix)
            suffix = suffix + logs[p]
    with jax.named_scope("tail_states"):
        for h in range(heads):
            own = slice(h * head, (h + 1) * head)
            w = jnp.concatenate([weighted[k, :, own] * decays[peers[k], :, own] for k in range(members)], axis=0)
            v = values[:, :, own].reshape(members * positions, head)
            state = sum(
                lax.dot_general(piece, v, (((0,), (0,)), ((), ())), preferred_element_type=F32)
                for piece in pieces(w, 2)
            )
            states[h] = state
            reads[me, :, own] = jnp.sum(query_down[h] * state, axis=0, keepdims=True)
    with jax.named_scope("sendreads"):
        for o in range(n - 1, 0, -1):
            read_copy(o, me).start()
    with jax.named_scope("tail_codes"):
        for h in range(heads):
            own = slice(h * head, (h + 1) * head)
            for g in range(group):
                span = slice(g * rows, (g + 1) * rows)
                codes[h, span], scales[g, :, own] = encode(states[h, span])
        for g in range(group):

            @pl.when(keeper(g) != me)
            def _():
                scale_copy(g).start()
                state_copy(g).start()

            @pl.when(keeper(g) == me)
            def _():
                got_codes[cube] = codes[:, g * rows : (g + 1) * rows]
                got_scales[cube] = scales[g]

    source = prompt_of(me // group)
    for c in range(cubes):

        @pl.when(c * members + source != me)
        @jax.named_scope("w_states")
        def _():
            for piece, arrived in ((got_scales.at[c], scale_recv.at[c]), (got_codes.at[c], state_recv.at[c])):
                pltpu.make_async_remote_copy(
                    src_ref=piece, dst_ref=piece,
                    send_sem=read_send, recv_sem=arrived,
                    device_id=(c * members + source, core), device_id_type=MESH,
                ).wait_recv()

    for h in range(heads):
        own = slice(h * head, (h + 1) * head)
        cache_out[h] = sum(decode(got_codes[c, h], got_scales[c, :, own]) for c in range(cubes)).astype(BF16)

    with jax.named_scope("w_reads"):
        all_reads.wait_recv()
    for s in range(s_count):
        row = jnp.zeros((1, width), F32)
        for c in range(cubes):
            row = row + reads[c * members + prompt_of(s)]
        sums[3, s : s + 1, :] = row
    for h in range(heads):
        lanes = slice(h * head, (h + 1) * head)
        mixed = sums[3, :, lanes] + jnp.sum(sums[0, :, lanes], axis=1, keepdims=True) * sums[1, :, lanes]
        normed = mixed * lax.rsqrt(jnp.mean(mixed * mixed, axis=1, keepdims=True) + EPSILON)
        read_out[:, lanes] = (normed * gains[...] * sums[2, :, lanes]).astype(BF16)

    all_keeps.wait_send()
    all_direct.wait_send()
    for o in range(1, t):
        token_copy(o, core).wait_send()
        many(blocks.at[pl.ds(1, members - 1), :, columns(core)], fwd_send.at[o - 1], read_recv).wait_send()
    all_early.wait_send()
    for g in range(group):

        @pl.when(keeper(g) != me)
        def _():
            scale_copy(g).wait_send()
            state_copy(g).wait_send()

    all_reads.wait_send()


def hand_over(cache, read, cache_out, read_out, sem):
    copies = [pltpu.make_async_copy(cache, cache_out, sem.at[0]), pltpu.make_async_copy(read, read_out, sem.at[1])]
    for copy in copies:
        copy.start()
    for copy in copies:
        copy.wait()


def per_device(prompt, keep_scale, new_token, w_query, w_forget, w_value, w_outgate, floor_gap, norm_gain):
    n, t = lax.axis_size("sp"), lax.axis_size("tp")
    s_count, positions, model = prompt.shape
    head = norm_gain.shape[0]
    width = w_forget.shape[1]
    heads = width // head
    members = s_count
    cubes = n // members
    group = cubes
    rows = head // group
    sizes = (n, t, s_count, members, cubes, heads, head, rows)
    dma = pltpu.SemaphoreType.DMA
    vmem = pl.BlockSpec(memory_space=pltpu.VMEM)
    hbm = pl.BlockSpec(memory_space=pltpu.HBM)
    cache, read = pl.pallas_call(
        functools.partial(kernel, sizes),
        out_shape=(
            pltpu.VMEM((heads, rows, head), BF16),
            pltpu.VMEM((s_count, width), BF16),
        ),
        in_specs=[hbm] * 9,
        out_specs=(vmem, vmem),
        scratch_shapes=[
            pltpu.VMEM((members, positions, model), BF16),
            pltpu.VMEM((members, positions, model), BF16),
            pltpu.VMEM((1,) + keep_scale.shape, F32),
            pltpu.VMEM((members - 1, 1, positions), F32),
            pltpu.VMEM((t,) + new_token.shape, BF16),
            pltpu.VMEM((model, width), BF16),
            pltpu.VMEM((3, model, width), BF16),
            pltpu.VMEM((1, width), F32),
            pltpu.VMEM((1, head), F32),
            pltpu.VMEM((members, positions, width), F32),
            pltpu.VMEM((members, positions, width), BF16),
            pltpu.VMEM((members, 1, width), F32),
            pltpu.VMEM((members, 1, width), F32),
            pltpu.VMEM((members, 1, width), F32),
            pltpu.VMEM((n, 1, width), F32),
            pltpu.VMEM((heads, head, head), F32),
            pltpu.VMEM((heads, head, head), BF16),
            pltpu.VMEM((group, 1, width), F32),
            pltpu.VMEM((cubes, heads, rows, head), BF16),
            pltpu.VMEM((cubes, 1, width), F32),
            pltpu.VMEM((n, 1, width), F32),
            pltpu.VMEM((4, s_count, width), F32),
            pltpu.VMEM((heads, head, head), F32),
            dma((7,)), dma((2,)), dma((t - 1,)),
            dma, dma((members // 2,)),
            dma, dma,
            dma((t - 1,)), dma((members // 2, t - 1)),
            dma((t - 1,)), dma((t - 1,)),
            dma, dma,
            dma((group,)), dma((cubes,)),
            dma((group,)), dma((cubes,)),
            dma, dma,
            pltpu.SemaphoreType.REGULAR,
        ],
        compiler_params=pltpu.CompilerParams(collective_id=0, has_side_effects=True, vmem_limit_bytes=32*1024*1024),
    )(
        *(
            pltpu.with_memory_space_constraint(x, pltpu.HBM)
            for x in (
                prompt, keep_scale, new_token, w_query, w_forget, w_value, w_outgate,
                floor_gap.reshape(1, width), norm_gain.reshape(1, head),
            )
        )
    )
    return pl.pallas_call(
        hand_over,
        out_shape=(
            jax.ShapeDtypeStruct((heads, rows, head), BF16),
            jax.ShapeDtypeStruct((s_count, width), BF16),
        ),
        in_specs=[vmem, vmem],
        out_specs=(pl.BlockSpec(memory_space=pltpu.HBM), pl.BlockSpec(memory_space=pltpu.HBM)),
        scratch_shapes=[dma((2,))],
        compiler_params=pltpu.CompilerParams(vmem_limit_bytes=1024*1024),
    )(cache, read)


def solution(mesh):
    return jax.shard_map(
        per_device,
        mesh=mesh,
        in_specs=(
            P(None, "sp", None),
            P(None, "sp"),
            P(None, "tp"),
            P(None, "tp"),
            P(None, "tp"),
            P(None, "tp"),
            P(None, "tp"),
            P("tp"),
            P(),
        ),
        out_specs=(P("tp", "sp", None), P(None, "tp")),
        check_vma=False,
    )
```

```python
import functools

import jax
import jax.numpy as jnp
from jax import lax
from jax.experimental import pallas as pl
from jax.experimental.pallas import tpu as pltpu
from jax.sharding import PartitionSpec as P

EPSILON = 1e-06
RANGE = 166.0
TINY = 1e-30
MESH = pl.DeviceIdType.MESH
F32 = jnp.float32
BF16 = jnp.bfloat16


def partner(mine, step, count):
    total, bit = mine, 1
    while bit < count:
        if step // bit % 2:
            total = total + bit * (1 - 2 * lax.rem(mine // bit, 2))
        bit *= 2
    return total


def pieces(x, count):
    out = []
    for _ in range(count):
        piece = x.astype(BF16)
        out.append(piece)
        x = x - piece.astype(F32)
    return out


def arrival_order(members):
    if members == 8:
        return (0, 7, 4, 2, 3, 5, 6, 1)
    return (0,) + tuple(range(members - 1, 0, -1))


def encode(x, most):
    level = jnp.exp(RANGE * (jnp.abs(x) * (1.0 / most) - 0.5))
    return jnp.where(x < 0.0, -level, level).astype(BF16)


def size_of(code):
    return jnp.log(jnp.abs(code.astype(F32))) * (1.0 / RANGE) + 0.5


def decode(code, most):
    size = size_of(code) * most
    return jnp.where(code.astype(F32) < 0.0, -size, size)


def column_most(x):
    return jnp.maximum(jnp.max(jnp.abs(x), axis=0, keepdims=True), TINY)


def kernel(
    sizes,
    prompt, keep, token, w_query, w_forget, w_value, w_outgate, floor, gain,
    cache_out, read_out,
    stage, raw, keeps, rows_in, tokens, wf, wv, weights, floors, gains,
    payload, landed, weighted, values, decays, mine_early, early, cross,
    states, codes, scales, got_codes, got_scales, reads, spare, sums, query_down,
    local_sem, stage_sem, other_sem, raw_send, raw_recv, keep_send, keep_recv, fwd_send, fwd_recv,
    pay_send, pay_recv, cross_send, cross_recv,
    token_send, token_recv, early_send, early_recv, scale_send, scale_recv, state_send, state_recv, read_send, read_recv,
    far_sem,
):
    n, t, s_count, members, cubes, heads, head, rows = sizes
    group = cubes
    me, core = lax.axis_index("sp"), lax.axis_index("tp")
    cube, place = me // members, lax.rem(me, members)
    model = prompt.shape[2]
    part = model // t
    positions = prompt.shape[1]
    width = heads * head
    order = arrival_order(members)
    half = members // 2

    def prompt_of(p):
        if members % 4:
            return p
        low = lax.rem(p, 4)
        return p - low + lax.rem(low, 2) * 2 + low // 2

    def columns(c):
        return pl.ds(pl.multiple_of(c * part, part), part)

    peers = [partner(place, r, members) for r in order]
    prompts = [prompt_of(p) for p in peers]
    mine = prompts[0]
    others = [lax.rem(core + o, t) for o in range(1, t)]

    def mate(k):
        return cube * members + peers[k], core

    def staging(k, c, sem):
        return pltpu.make_async_copy(prompt.at[prompts[k], :, columns(c)], stage.at[k, :, columns(c)], sem)

    def sent(c):
        return stage.at[pl.ds(1, half - 1), :, columns(c)]

    def whole(k, sem):
        return pltpu.make_async_copy(prompt.at[prompts[k]], stage.at[k], sem)

    local = [
        pltpu.make_async_copy(keep, keeps.at[0], local_sem.at[0]),
        pltpu.make_async_copy(token, tokens.at[core], local_sem.at[1]),
        pltpu.make_async_copy(floor, floors, local_sem.at[2]),
        pltpu.make_async_copy(gain, gains, local_sem.at[3]),
        pltpu.make_async_copy(w_forget, wf, local_sem.at[4]),
        pltpu.make_async_copy(w_value, wv, local_sem.at[5]),
        pltpu.make_async_copy(w_query, weights.at[0], local_sem.at[6]),
        pltpu.make_async_copy(w_outgate, weights.at[1], local_sem.at[6]),
    ]

    for k in range(1, half):
        staging(k, core, stage_sem.at[0]).start()
    barrier = pltpu.get_barrier_semaphore()
    for k in range(1, members):
        pl.semaphore_signal(barrier, inc=1, device_id=mate(k), device_id_type=MESH)
    for o in range(1, cubes):
        pl.semaphore_signal(barrier, inc=1, device_id=(lax.rem(me + o * members, n), core), device_id_type=MESH)
    for o in range(1, t):
        pl.semaphore_signal(barrier, inc=1, device_id=(me, lax.rem(core + o, t)), device_id_type=MESH)
    local[0].start()
    local[2].start()
    local[4].start()
    for k in range(half, half + 2):
        whole(k, stage_sem.at[1]).start()
    local[5].start()
    for k in range(half + 2, members):
        whole(k, stage_sem.at[2]).start()
    whole(0, stage_sem.at[2]).start()
    for i, c in enumerate(others):
        for k in range(1, half):
            staging(k, c, other_sem.at[i]).start()
    for i in (1, 3, 6, 7):
        local[i].start()

    def raw_copy(k):
        return pltpu.make_async_remote_copy(
            src_ref=stage.at[k, :, columns(core)], dst_ref=raw.at[k - 1, :, columns(core)],
            send_sem=raw_send, recv_sem=raw_recv, device_id=mate(k), device_id_type=MESH,
        )

    def keep_copy(k):
        return pltpu.make_async_remote_copy(
            src_ref=keeps.at[0, pl.ds(prompts[k], 1)], dst_ref=rows_in.at[k - 1],
            send_sem=keep_send, recv_sem=keep_recv, device_id=mate(k), device_id_type=MESH,
        )

    def forward(o, c):
        piece = raw.at[:, :, columns(c)]
        return pltpu.make_async_remote_copy(
            src_ref=piece, dst_ref=piece,
            send_sem=fwd_send.at[o - 1], recv_sem=fwd_recv.at[o - 1],
            device_id=(me, lax.rem(core + o, t)), device_id_type=MESH,
        )

    def pay_copy(k):
        return pltpu.make_async_remote_copy(
            src_ref=payload.at[k - half], dst_ref=landed.at[k - half],
            send_sem=pay_send, recv_sem=pay_recv.at[(k - half) // 2],
            device_id=mate(k), device_id_type=MESH,
        )

    def token_copy(o, c):
        return pltpu.make_async_remote_copy(
            src_ref=tokens.at[c], dst_ref=tokens.at[c],
            send_sem=token_send.at[o - 1], recv_sem=token_recv.at[o - 1],
            device_id=(me, lax.rem(core + o, t)), device_id_type=MESH,
        )

    def early_copy(k):
        return pltpu.make_async_remote_copy(
            src_ref=mine_early.at[k], dst_ref=early.at[place],
            send_sem=early_send, recv_sem=early_recv,
            device_id=mate(k), device_id_type=MESH,
        )

    def cross_copy(c, k):
        return pltpu.make_async_remote_copy(
            src_ref=mine_early.at[k, 0], dst_ref=cross.at[cube, place],
            send_sem=cross_send.at[c], recv_sem=cross_recv.at[cube],
            device_id=(c * members + peers[k], core), device_id_type=MESH,
        )

    def keeper(g):
        return mine * group + g

    def scale_copy(g):
        return pltpu.make_async_remote_copy(
            src_ref=scales.at[g], dst_ref=got_scales.at[cube],
            send_sem=scale_send.at[g], recv_sem=scale_recv.at[cube],
            device_id=(keeper(g), core), device_id_type=MESH,
        )

    def state_copy(g):
        return pltpu.make_async_remote_copy(
            src_ref=codes.at[:, pl.ds(g * rows, rows), :],
            dst_ref=got_codes.at[cube],
            send_sem=state_send.at[g], recv_sem=state_recv.at[cube],
            device_id=(keeper(g), core), device_id_type=MESH,
        )

    def read_copy(o):
        piece = reads.at[cube, pl.ds(mine, 1)]
        return pltpu.make_async_remote_copy(
            src_ref=piece, dst_ref=piece,
            send_sem=read_send, recv_sem=read_recv,
            device_id=(lax.rem(me + o, n), core), device_id_type=MESH,
        )

    def many(ref, send, recv):
        return pltpu.make_async_remote_copy(
            src_ref=ref, dst_ref=ref, send_sem=send, recv_sem=recv,
            device_id=(lax.rem(me + 1, n), core), device_id_type=MESH,
        )

    all_raw = many(raw.at[:, :, columns(core)], raw_send, raw_recv)
    all_keeps = many(rows_in, keep_send, keep_recv)
    all_pay = many(landed, pay_send, pay_recv.at[0])
    all_early = many(early.at[pl.ds(0, members - 1)], early_send, early_recv)
    all_reads = many(spare, read_send, read_recv)

    with jax.named_scope("barrier"):
        pl.semaphore_wait(barrier, members - 1 + cubes - 1 + t - 1)
    pltpu.make_async_copy(sent(core), sent(core), stage_sem.at[0]).wait()
    for k in range(1, half):
        raw_copy(k).start()
    local[0].wait()
    for k in range(1, half):
        keep_copy(k).start()
    for k in range(1, members):
        pl.semaphore_signal(far_sem, inc=1, device_id=mate(k), device_id_type=MESH)

    with jax.named_scope("wlocal"):
        local[2].wait()
        local[4].wait()
        both = stage.at[pl.ds(half, 2)]
        pltpu.make_async_copy(both, both, stage_sem.at[1]).wait()
    floor_row = floors[...]
    p0 = lax.broadcasted_iota(jnp.int32, (positions, positions), 0)
    p1 = lax.broadcasted_iota(jnp.int32, (positions, positions), 1)

    def column(row):
        return jnp.sum(jnp.where(p0 == p1, jnp.broadcast_to(row, (positions, positions)), 0.0), axis=1, keepdims=True)

    def value(x):
        return jnp.dot(x, wv[...], preferred_element_type=F32).astype(BF16)

    def forget(x, keep_rows):
        size = x.shape[0]
        pre = jnp.dot(x, wf[...], preferred_element_type=F32)
        loss = floor_row * (1.0 / (1.0 + jnp.exp(pre)))
        scale = jnp.concatenate([column(row) for row in keep_rows], axis=0)
        log_forget = jnp.log(scale * (1.0 - loss))
        gate = 1.0 - scale + scale * loss
        j0 = lax.broadcasted_iota(jnp.int32, (size, size), 0)
        j1 = lax.broadcasted_iota(jnp.int32, (size, size), 1)
        later = jnp.where((j1 > j0) & (j0 // positions == j1 // positions), 1.0, 0.0).astype(BF16)
        inside = sum(jnp.dot(later, piece, preferred_element_type=F32) for piece in pieces(log_forget, 2))
        totals = [
            inside[first : first + 1] + log_forget[first : first + 1] for first in range(0, size, positions)
        ]
        return gate * jnp.exp(inside), totals

    def kept(k):
        return keeps[0, pl.ds(prompts[k], 1), :]

    def prepare(k):
        x = stage[k : k + 2].reshape(2 * positions, model)
        key, totals = forget(x, [kept(k), kept(k + 1)])
        if k == half:
            local[5].wait()
        fresh = value(x)
        for i in range(2):
            span = slice(i * positions, (i + 1) * positions)
            most = column_most(key[span])
            payload[k + i - half, :, :width] = encode(key[span], most)
            payload[k + i - half, :, width:] = fresh[span]
            mine_early[k + i, 0] = totals[i]
            mine_early[k + i, 1] = most

    with jax.named_scope("prepare"):
        for k in range(half, members, 2):
            if k > half:
                rest = stage.at[pl.ds(half + 1, half - 1)]
                pltpu.make_async_copy(rest, rest, stage_sem.at[2]).wait()
            prepare(k)
            if k == half:
                pay_copy(k).start()
                pay_copy(k + 1).start()
    with jax.named_scope("own"):
        for i, c in enumerate(others):
            pltpu.make_async_copy(sent(c), sent(c), other_sem.at[i]).wait()
        x = stage[0:half].reshape(half * positions, model)
        key, totals = forget(x, [kept(k) for k in range(half)])
        weighted[0] = key[:positions]
        for k in range(half):
            mine_early[k, 0] = totals[k]
            mine_early[k, 1] = totals[k]
        early[place, 0] = totals[0]
        pl.semaphore_wait(far_sem, members - 1)
        for c in range(cubes - 1):

            @pl.when(c < cube)
            def _():
                for k in range(members):
                    cross_copy(c, k).start()

        for k in range(1, members):
            early_copy(k).start()
        values[0] = value(stage[0])

    with jax.named_scope("wlocal2"):
        local[1].wait()
        for o in range(1, t):
            token_copy(o, core).start()
        local[3].wait()
        pltpu.make_async_copy(weights, weights, local_sem.at[6]).wait()
        for o in range(1, t):
            token_copy(o, lax.rem(core - o + t, t)).wait_recv()
    with jax.named_scope("token"):
        feature = jnp.concatenate([tokens[c] for c in range(t)], axis=1)
        query = jnp.dot(feature, weights[0], preferred_element_type=F32)
        new_forget = jnp.dot(feature, wf[...], preferred_element_type=F32)
        new_value = jnp.dot(feature, wv[...], preferred_element_type=F32).astype(BF16).astype(F32)
        new_gate = jnp.dot(feature, weights[1], preferred_element_type=F32)
        new_loss = floor_row * (1.0 / (1.0 + jnp.exp(new_forget)))
        read_weight = query * (1.0 - new_loss)
        silu = new_gate * (1.0 / (1.0 + jnp.exp(-new_gate)))
        fresh = query * new_loss
        for h in range(heads):
            own = slice(h * head, (h + 1) * head)
            sums[0, :, own] = jnp.sum(fresh[:, own], axis=1, keepdims=True) * new_value[:, own]
            sums[1, :, own] = gains[...] * silu[:, own]
        seq = lax.broadcasted_iota(jnp.int32, read_weight.shape, 0)
        picked = jnp.where(seq == mine, read_weight, 0.0)
        weight = jnp.sum(picked, axis=0, keepdims=True)
        h0 = lax.broadcasted_iota(jnp.int32, (head, head), 0)
        h1 = lax.broadcasted_iota(jnp.int32, (head, head), 1)
        for h in range(heads):
            row = jnp.broadcast_to(weight[:, h * head : (h + 1) * head], (head, head))
            down = jnp.sum(jnp.where(h0 == h1, row, 0.0), axis=1, keepdims=True)
            query_down[h] = jnp.broadcast_to(down, (head, head))

    def add_up(first, last, start):
        found = []
        for h in range(heads):
            own = slice(h * head, (h + 1) * head)
            keys, fresh = [], []
            for k in range(first, last):
                decay = decays[peers[k], :, own]
                if k < half:
                    keys.append(weighted[k, :, own] * decay)
                    fresh.append(values[k, :, own])
                else:
                    keys.append(size_of(landed[k - half, :, own]) * (early[peers[k], 1, :, own] * decay))
                    fresh.append(landed[k - half, :, width + h * head : width + (h + 1) * head])
            keys, fresh = jnp.concatenate(keys, axis=0), jnp.concatenate(fresh, axis=0)
            state = sum(
                lax.dot_general(piece, fresh, (((0,), (0,)), ((), ())), preferred_element_type=F32)
                for piece in pieces(keys, 2)
            )
            state = state if start else states[h] + state
            states[h] = state
            found.append(jnp.sum(query_down[h] * state, axis=0, keepdims=True))
        return found

    def arrive(j):
        with jax.named_scope("w_pay"):
            many(landed.at[pl.ds(2 * j, 2)], pay_send, pay_recv.at[j]).wait_recv()

    for k in range(half + 2, members):
        pay_copy(k).start()
    with jax.named_scope("w_raw"):
        all_raw.wait_recv()
        for o in range(1, t):
            forward(o, core).start()
        all_keeps.wait_recv()
        for o in range(1, t):
            forward(o, lax.rem(core - o + t, t)).wait_recv()
    with jax.named_scope("raw"):
        x = raw[...].reshape((half - 1) * positions, model)
        key, _ = forget(x, [rows_in[k] for k in range(half - 1)])
        weighted[1:half] = key.reshape(half - 1, positions, width)
        values[1:half] = value(x).reshape(half - 1, positions, width)
    with jax.named_scope("w_early"):
        all_early.wait_recv()
        for c in range(1, cubes):

            @pl.when(c > cube)
            def _():
                many(cross.at[c], cross_send.at[0], cross_recv.at[c]).wait_recv()

            @pl.when(c <= cube)
            def _():
                cross[c] = jnp.zeros((members, 1, width), F32)

    with jax.named_scope("decays"):
        suffix = jnp.zeros((1, width), F32)
        for c in range(1, cubes):
            for p in range(members):
                suffix = suffix + cross[c, p]
        for p in reversed(range(members)):
            decays[p] = jnp.exp(suffix)
            suffix = suffix + early[p, 0]
    tail = half // 2 - 1
    for j in range(tail):
        arrive(j)
    with jax.named_scope("states"):
        add_up(0, members - 2, True)
    arrive(tail)
    with jax.named_scope("tail_states"):
        found = add_up(members - 2, members, False)
        reads[cube, pl.ds(mine, 1), :] = jnp.concatenate(found, axis=1)
    with jax.named_scope("sendreads"):
        for o in range(n - 1, 0, -1):
            read_copy(o).start()
    with jax.named_scope("tail_codes"):
        for h in range(heads):
            own = slice(h * head, (h + 1) * head)
            for g in range(group):
                span = slice(g * rows, (g + 1) * rows)
                most = column_most(states[h, span])
                codes[h, span], scales[g, :, own] = encode(states[h, span], most), most
        for g in range(group):

            @pl.when(keeper(g) != me)
            def _():
                scale_copy(g).start()
                state_copy(g).start()

            @pl.when(keeper(g) == me)
            def _():
                got_codes[cube] = codes[:, g * rows : (g + 1) * rows]
                got_scales[cube] = scales[g]

    source = prompt_of(me // group)
    for c in range(cubes):

        @pl.when(c * members + source != me)
        @jax.named_scope("w_states")
        def _():
            for piece, arrived in ((got_scales.at[c], scale_recv.at[c]), (got_codes.at[c], state_recv.at[c])):
                pltpu.make_async_remote_copy(
                    src_ref=piece, dst_ref=piece,
                    send_sem=read_send, recv_sem=arrived,
                    device_id=(c * members + source, core), device_id_type=MESH,
                ).wait_recv()

    for h in range(heads):
        own = slice(h * head, (h + 1) * head)
        cache_out[h] = sum(decode(got_codes[c, h], got_scales[c, :, own]) for c in range(cubes)).astype(BF16)

    with jax.named_scope("w_reads"):
        all_reads.wait_recv()
    mixed = sums[0]
    for c in range(cubes):
        mixed = mixed + reads[c]
    for h in range(heads):
        own = slice(h * head, (h + 1) * head)
        part_mixed = mixed[:, own]
        spread = lax.rsqrt(jnp.mean(part_mixed * part_mixed, axis=1, keepdims=True) + EPSILON)
        read_out[:, own] = (part_mixed * spread * sums[1, :, own]).astype(BF16)

    all_raw.wait_send()
    all_keeps.wait_send()
    all_pay.wait_send()
    for o in range(1, t):
        token_copy(o, core).wait_send()
        forward(o, core).wait_send()
    all_early.wait_send()
    for c in range(cubes - 1):

        @pl.when(c < cube)
        def _():
            many(cross.at[0], cross_send.at[c], early_recv).wait_send()

    for g in range(group):

        @pl.when(keeper(g) != me)
        def _():
            scale_copy(g).wait_send()
            state_copy(g).wait_send()

    all_reads.wait_send()


def hand_over(cache, read, cache_out, read_out, sem):
    copies = [pltpu.make_async_copy(cache, cache_out, sem.at[0]), pltpu.make_async_copy(read, read_out, sem.at[1])]
    for copy in copies:
        copy.start()
    for copy in copies:
        copy.wait()


def per_device(prompt, keep_scale, new_token, w_query, w_forget, w_value, w_outgate, floor_gap, norm_gain):
    n, t = lax.axis_size("sp"), lax.axis_size("tp")
    s_count, positions, model = prompt.shape
    head = norm_gain.shape[0]
    width = w_forget.shape[1]
    heads = width // head
    members = s_count
    cubes = n // members
    group = cubes
    rows = head // group
    sizes = (n, t, s_count, members, cubes, heads, head, rows)
    dma = pltpu.SemaphoreType.DMA
    vmem = pl.BlockSpec(memory_space=pltpu.VMEM)
    hbm = pl.BlockSpec(memory_space=pltpu.HBM)
    cache, read = pl.pallas_call(
        functools.partial(kernel, sizes),
        out_shape=(
            pltpu.VMEM((heads, rows, head), BF16),
            pltpu.VMEM((s_count, width), BF16),
        ),
        in_specs=[hbm] * 9,
        out_specs=(vmem, vmem),
        scratch_shapes=[
            pltpu.VMEM((members, positions, model), BF16),
            pltpu.VMEM((members // 2 - 1, positions, model), BF16),
            pltpu.VMEM((1,) + keep_scale.shape, F32),
            pltpu.VMEM((members // 2 - 1, 1, positions), F32),
            pltpu.VMEM((t,) + new_token.shape, BF16),
            pltpu.VMEM((model, width), BF16),
            pltpu.VMEM((model, width), BF16),
            pltpu.VMEM((2, model, width), BF16),
            pltpu.VMEM((1, width), F32),
            pltpu.VMEM((1, head), F32),
            pltpu.VMEM((members // 2, positions, 2 * width), BF16),
            pltpu.VMEM((members // 2, positions, 2 * width), BF16),
            pltpu.VMEM((members // 2, positions, width), F32),
            pltpu.VMEM((members // 2, positions, width), BF16),
            pltpu.VMEM((members, 1, width), F32),
            pltpu.VMEM((members, 2, 1, width), F32),
            pltpu.VMEM((members, 2, 1, width), F32),
            pltpu.VMEM((cubes, members, 1, width), F32),
            pltpu.VMEM((heads, head, head), F32),
            pltpu.VMEM((heads, head, head), BF16),
            pltpu.VMEM((group, 1, width), F32),
            pltpu.VMEM((cubes, heads, rows, head), BF16),
            pltpu.VMEM((cubes, 1, width), F32),
            pltpu.VMEM((cubes, s_count, width), F32),
            pltpu.VMEM((n - 1, 1, width), F32),
            pltpu.VMEM((2, s_count, width), F32),
            pltpu.VMEM((heads, head, head), F32),
            dma((7,)), dma((3,)), dma((t - 1,)),
            dma, dma, dma, dma,
            dma((t - 1,)), dma((t - 1,)),
            dma, dma((members // 4,)),
            dma((cubes - 1,)), dma((cubes,)),
            dma((t - 1,)), dma((t - 1,)),
            dma, dma,
            dma((group,)), dma((cubes,)),
            dma((group,)), dma((cubes,)),
            dma, dma,
            pltpu.SemaphoreType.REGULAR,
        ],
        compiler_params=pltpu.CompilerParams(collective_id=0, has_side_effects=True, vmem_limit_bytes=32*1024*1024),
    )(
        *(
            pltpu.with_memory_space_constraint(x, pltpu.HBM)
            for x in (
                prompt, keep_scale, new_token, w_query, w_forget, w_value, w_outgate,
                floor_gap.reshape(1, width), norm_gain.reshape(1, head),
            )
        )
    )
    return pl.pallas_call(
        hand_over,
        out_shape=(
            jax.ShapeDtypeStruct((heads, rows, head), BF16),
            jax.ShapeDtypeStruct((s_count, width), BF16),
        ),
        in_specs=[vmem, vmem],
        out_specs=(pl.BlockSpec(memory_space=pltpu.HBM), pl.BlockSpec(memory_space=pltpu.HBM)),
        scratch_shapes=[dma((2,))],
        compiler_params=pltpu.CompilerParams(vmem_limit_bytes=1024*1024),
    )(cache, read)


def solution(mesh):
    return jax.shard_map(
        per_device,
        mesh=mesh,
        in_specs=(
            P(None, "sp", None),
            P(None, "sp"),
            P(None, "tp"),
            P(None, "tp"),
            P(None, "tp"),
            P(None, "tp"),
            P(None, "tp"),
            P("tp"),
            P(),
        ),
        out_specs=(P("tp", "sp", None), P(None, "tp")),
        check_vma=False,
    )
```

```python
import functools

import jax
import jax.numpy as jnp
from jax import lax
from jax.experimental import pallas as pl
from jax.experimental.pallas import tpu as pltpu
from jax.sharding import PartitionSpec as P

EPSILON = 1e-06
RANGE = 166.0
TINY = 1e-30
MESH = pl.DeviceIdType.MESH
F32 = jnp.float32
BF16 = jnp.bfloat16


def partner(mine, step, count):
    total, bit = mine, 1
    while bit < count:
        if step // bit % 2:
            total = total + bit * (1 - 2 * lax.rem(mine // bit, 2))
        bit *= 2
    return total


def pieces(x, count):
    out = []
    for _ in range(count):
        piece = x.astype(BF16)
        out.append(piece)
        x = x - piece.astype(F32)
    return out


def arrival_order(members):
    if members == 8:
        return (0, 7, 4, 2, 3, 5, 6, 1)
    return (0,) + tuple(range(members - 1, 0, -1))


def encode(x, most):
    level = jnp.exp(RANGE * (jnp.abs(x) * (1.0 / most) - 0.5))
    return jnp.where(x < 0.0, -level, level).astype(BF16)


def encode_key(x, most):
    return jnp.exp(RANGE * (jnp.sqrt(jnp.sqrt(jnp.maximum(x * (1.0 / most), TINY))) - 0.5)).astype(BF16)


def key_of(code):
    root = size_of(code)
    return (root * root) * (root * root)


def size_of(code):
    return jnp.log(jnp.abs(code.astype(F32))) * (1.0 / RANGE) + 0.5


def decode(code, most):
    size = size_of(code) * most
    return jnp.where(code.astype(F32) < 0.0, -size, size)


def column_most(x):
    return jnp.maximum(jnp.max(jnp.abs(x), axis=0, keepdims=True), TINY)


def kernel(
    sizes,
    prompt, keep, token, w_query, w_forget, w_value, w_outgate, floor, gain,
    cache_out, read_out,
    stage, raw, keeps, rows_in, tokens, wf, wv, weights, floors, gains,
    payload, landed, weighted, values, decays, mine_early, early, cross,
    states, codes, scales, got_codes, got_scales, reads, spare, sums, query_down,
    local_sem, stage_sem, other_sem, raw_send, raw_recv, keep_send, keep_recv, fwd_send, fwd_recv,
    pay_send, pay_recv, cross_send, cross_recv,
    token_send, token_recv, early_send, early_recv, scale_send, scale_recv, state_send, state_recv, read_send, read_recv,
    far_sem,
):
    n, t, s_count, members, cubes, heads, head, rows = sizes
    group = cubes
    me, core = lax.axis_index("sp"), lax.axis_index("tp")
    cube, place = me // members, lax.rem(me, members)
    model = prompt.shape[2]
    part = model // t
    positions = prompt.shape[1]
    width = heads * head
    order = arrival_order(members)
    half = members // 2

    def prompt_of(p):
        if members % 4:
            return p
        low = lax.rem(p, 4)
        return p - low + lax.rem(low, 2) * 2 + low // 2

    def columns(c):
        return pl.ds(pl.multiple_of(c * part, part), part)

    peers = [partner(place, r, members) for r in order]
    prompts = [prompt_of(p) for p in peers]
    mine = prompts[0]
    others = [lax.rem(core + o, t) for o in range(1, t)]

    def mate(k):
        return cube * members + peers[k], core

    def staging(k, c, sem):
        return pltpu.make_async_copy(prompt.at[prompts[k], :, columns(c)], stage.at[k, :, columns(c)], sem)

    def sent(c):
        return stage.at[pl.ds(1, half - 1), :, columns(c)]

    def whole(k, sem):
        return pltpu.make_async_copy(prompt.at[prompts[k]], stage.at[k], sem)

    local = [
        pltpu.make_async_copy(keep, keeps.at[0], local_sem.at[0]),
        pltpu.make_async_copy(token, tokens.at[core], local_sem.at[1]),
        pltpu.make_async_copy(floor, floors, local_sem.at[2]),
        pltpu.make_async_copy(gain, gains, local_sem.at[3]),
        pltpu.make_async_copy(w_forget, wf, local_sem.at[4]),
        pltpu.make_async_copy(w_value, wv, local_sem.at[5]),
        pltpu.make_async_copy(w_query, weights.at[0], local_sem.at[6]),
        pltpu.make_async_copy(w_outgate, weights.at[1], local_sem.at[6]),
    ]

    for k in range(1, half):
        staging(k, core, stage_sem.at[0]).start()
    barrier = pltpu.get_barrier_semaphore()
    for k in range(1, members):
        pl.semaphore_signal(barrier, inc=1, device_id=mate(k), device_id_type=MESH)
    for o in range(1, cubes):
        pl.semaphore_signal(barrier, inc=1, device_id=(lax.rem(me + o * members, n), core), device_id_type=MESH)
    for o in range(1, t):
        pl.semaphore_signal(barrier, inc=1, device_id=(me, lax.rem(core + o, t)), device_id_type=MESH)
    local[0].start()
    local[2].start()
    local[4].start()
    for k in range(half, half + 2):
        whole(k, stage_sem.at[1]).start()
    local[5].start()
    for k in range(half + 2, members):
        whole(k, stage_sem.at[2]).start()
    whole(0, stage_sem.at[2]).start()
    for i, c in enumerate(others):
        for k in range(1, half):
            staging(k, c, other_sem.at[i]).start()
    for i in (1, 3, 6, 7):
        local[i].start()

    def raw_copy(k):
        return pltpu.make_async_remote_copy(
            src_ref=stage.at[k, :, columns(core)], dst_ref=raw.at[k - 1, :, columns(core)],
            send_sem=raw_send, recv_sem=raw_recv, device_id=mate(k), device_id_type=MESH,
        )

    def keep_copy(k):
        return pltpu.make_async_remote_copy(
            src_ref=keeps.at[0, pl.ds(prompts[k], 1)], dst_ref=rows_in.at[k - 1],
            send_sem=keep_send, recv_sem=keep_recv, device_id=mate(k), device_id_type=MESH,
        )

    def forward(o, c):
        piece = raw.at[:, :, columns(c)]
        return pltpu.make_async_remote_copy(
            src_ref=piece, dst_ref=piece,
            send_sem=fwd_send.at[o - 1], recv_sem=fwd_recv.at[o - 1],
            device_id=(me, lax.rem(core + o, t)), device_id_type=MESH,
        )

    def pay_copy(k):
        return pltpu.make_async_remote_copy(
            src_ref=payload.at[k - half], dst_ref=landed.at[k - half],
            send_sem=pay_send, recv_sem=pay_recv.at[(k - half) // 2],
            device_id=mate(k), device_id_type=MESH,
        )

    def token_copy(o, c):
        return pltpu.make_async_remote_copy(
            src_ref=tokens.at[c], dst_ref=tokens.at[c],
            send_sem=token_send.at[o - 1], recv_sem=token_recv.at[o - 1],
            device_id=(me, lax.rem(core + o, t)), device_id_type=MESH,
        )

    def early_copy(k):
        return pltpu.make_async_remote_copy(
            src_ref=mine_early.at[k], dst_ref=early.at[place],
            send_sem=early_send, recv_sem=early_recv,
            device_id=mate(k), device_id_type=MESH,
        )

    def cross_copy(c, k):
        return pltpu.make_async_remote_copy(
            src_ref=mine_early.at[k, 0], dst_ref=cross.at[cube, place],
            send_sem=cross_send.at[c], recv_sem=cross_recv.at[cube],
            device_id=(c * members + peers[k], core), device_id_type=MESH,
        )

    def keeper(g):
        return mine * group + g

    def scale_copy(g):
        return pltpu.make_async_remote_copy(
            src_ref=scales.at[g], dst_ref=got_scales.at[cube],
            send_sem=scale_send.at[g], recv_sem=scale_recv.at[cube],
            device_id=(keeper(g), core), device_id_type=MESH,
        )

    def state_copy(g):
        return pltpu.make_async_remote_copy(
            src_ref=codes.at[:, pl.ds(g * rows, rows), :],
            dst_ref=got_codes.at[cube],
            send_sem=state_send.at[g], recv_sem=state_recv.at[cube],
            device_id=(keeper(g), core), device_id_type=MESH,
        )

    def read_copy(o):
        piece = reads.at[cube, pl.ds(mine, 1)]
        return pltpu.make_async_remote_copy(
            src_ref=piece, dst_ref=piece,
            send_sem=read_send, recv_sem=read_recv,
            device_id=(lax.rem(me + o, n), core), device_id_type=MESH,
        )

    def many(ref, send, recv):
        return pltpu.make_async_remote_copy(
            src_ref=ref, dst_ref=ref, send_sem=send, recv_sem=recv,
            device_id=(lax.rem(me + 1, n), core), device_id_type=MESH,
        )

    all_raw = many(raw.at[:, :, columns(core)], raw_send, raw_recv)
    all_keeps = many(rows_in, keep_send, keep_recv)
    all_pay = many(landed, pay_send, pay_recv.at[0])
    all_early = many(early.at[pl.ds(0, members - 1)], early_send, early_recv)
    all_reads = many(spare, read_send, read_recv)

    with jax.named_scope("barrier"):
        pl.semaphore_wait(barrier, members - 1 + cubes - 1 + t - 1)
    pltpu.make_async_copy(sent(core), sent(core), stage_sem.at[0]).wait()
    for k in range(1, half):
        raw_copy(k).start()
    local[0].wait()
    for k in range(1, half):
        keep_copy(k).start()
    for k in range(1, members):
        pl.semaphore_signal(far_sem, inc=1, device_id=mate(k), device_id_type=MESH)

    with jax.named_scope("wlocal"):
        local[2].wait()
        local[4].wait()
        both = stage.at[pl.ds(half, 2)]
        pltpu.make_async_copy(both, both, stage_sem.at[1]).wait()
    floor_row = floors[...]
    p0 = lax.broadcasted_iota(jnp.int32, (positions, positions), 0)
    p1 = lax.broadcasted_iota(jnp.int32, (positions, positions), 1)

    def column(row):
        return jnp.sum(jnp.where(p0 == p1, jnp.broadcast_to(row, (positions, positions)), 0.0), axis=1, keepdims=True)

    def value(x):
        return jnp.dot(x, wv[...], preferred_element_type=F32).astype(BF16)

    def forget(x, keep_rows):
        size = x.shape[0]
        pre = jnp.dot(x, wf[...], preferred_element_type=F32)
        loss = floor_row * (1.0 / (1.0 + jnp.exp(pre)))
        scale = jnp.concatenate([column(row) for row in keep_rows], axis=0)
        log_forget = jnp.log(scale * (1.0 - loss))
        gate = 1.0 - scale + scale * loss
        j0 = lax.broadcasted_iota(jnp.int32, (size, size), 0)
        j1 = lax.broadcasted_iota(jnp.int32, (size, size), 1)
        later = jnp.where((j1 > j0) & (j0 // positions == j1 // positions), 1.0, 0.0).astype(BF16)
        inside = sum(jnp.dot(later, piece, preferred_element_type=F32) for piece in pieces(log_forget, 2))
        totals = [
            inside[first : first + 1] + log_forget[first : first + 1] for first in range(0, size, positions)
        ]
        return gate * jnp.exp(inside), totals

    def kept(k):
        return keeps[0, pl.ds(prompts[k], 1), :]

    def prepare(k):
        x = stage[k : k + 2].reshape(2 * positions, model)
        key, totals = forget(x, [kept(k), kept(k + 1)])
        if k == half:
            local[5].wait()
        fresh = value(x)
        for i in range(2):
            span = slice(i * positions, (i + 1) * positions)
            most = column_most(key[span])
            payload[k + i - half, :, :width] = encode_key(key[span], most)
            payload[k + i - half, :, width:] = fresh[span]
            mine_early[k + i, 0] = totals[i]
            mine_early[k + i, 1] = most

    with jax.named_scope("prepare"):
        for k in range(half, members, 2):
            if k > half:
                rest = stage.at[pl.ds(half + 1, half - 1)]
                pltpu.make_async_copy(rest, rest, stage_sem.at[2]).wait()
            prepare(k)
            if k == half:
                pay_copy(k).start()
                pay_copy(k + 1).start()
    with jax.named_scope("own"):
        for i, c in enumerate(others):
            pltpu.make_async_copy(sent(c), sent(c), other_sem.at[i]).wait()
        x = stage[0:half].reshape(half * positions, model)
        key, totals = forget(x, [kept(k) for k in range(half)])
        weighted[0] = key[:positions]
        for k in range(half):
            mine_early[k, 0] = totals[k]
            mine_early[k, 1] = totals[k]
        early[place, 0] = totals[0]
        pl.semaphore_wait(far_sem, members - 1)
        for c in range(cubes - 1):

            @pl.when(c < cube)
            def _():
                for k in range(members):
                    cross_copy(c, k).start()

        for k in range(1, members):
            early_copy(k).start()
        values[0] = value(stage[0])

    with jax.named_scope("wlocal2"):
        local[1].wait()
        for o in range(1, t):
            token_copy(o, core).start()
        local[3].wait()
        pltpu.make_async_copy(weights, weights, local_sem.at[6]).wait()
        for o in range(1, t):
            token_copy(o, lax.rem(core - o + t, t)).wait_recv()
    with jax.named_scope("token"):
        feature = jnp.concatenate([tokens[c] for c in range(t)], axis=1)
        query = jnp.dot(feature, weights[0], preferred_element_type=F32)
        new_forget = jnp.dot(feature, wf[...], preferred_element_type=F32)
        new_value = jnp.dot(feature, wv[...], preferred_element_type=F32).astype(BF16).astype(F32)
        new_gate = jnp.dot(feature, weights[1], preferred_element_type=F32)
        new_loss = floor_row * (1.0 / (1.0 + jnp.exp(new_forget)))
        read_weight = query * (1.0 - new_loss)
        silu = new_gate * (1.0 / (1.0 + jnp.exp(-new_gate)))
        fresh = query * new_loss
        for h in range(heads):
            own = slice(h * head, (h + 1) * head)
            sums[0, :, own] = jnp.sum(fresh[:, own], axis=1, keepdims=True) * new_value[:, own]
            sums[1, :, own] = gains[...] * silu[:, own]
        seq = lax.broadcasted_iota(jnp.int32, read_weight.shape, 0)
        picked = jnp.where(seq == mine, read_weight, 0.0)
        weight = jnp.sum(picked, axis=0, keepdims=True)
        h0 = lax.broadcasted_iota(jnp.int32, (head, head), 0)
        h1 = lax.broadcasted_iota(jnp.int32, (head, head), 1)
        for h in range(heads):
            row = jnp.broadcast_to(weight[:, h * head : (h + 1) * head], (head, head))
            down = jnp.sum(jnp.where(h0 == h1, row, 0.0), axis=1, keepdims=True)
            query_down[h] = jnp.broadcast_to(down, (head, head))

    def add_up(first, last, start):
        found = []
        for h in range(heads):
            own = slice(h * head, (h + 1) * head)
            keys, fresh = [], []
            for k in range(first, last):
                decay = decays[peers[k], :, own]
                if k < half:
                    keys.append(weighted[k, :, own] * decay)
                    fresh.append(values[k, :, own])
                else:
                    keys.append(key_of(landed[k - half, :, own]) * (early[peers[k], 1, :, own] * decay))
                    fresh.append(landed[k - half, :, width + h * head : width + (h + 1) * head])
            keys, fresh = jnp.concatenate(keys, axis=0), jnp.concatenate(fresh, axis=0)
            state = sum(
                lax.dot_general(piece, fresh, (((0,), (0,)), ((), ())), preferred_element_type=F32)
                for piece in pieces(keys, 2)
            )
            state = state if start else states[h] + state
            states[h] = state
            found.append(jnp.sum(query_down[h] * state, axis=0, keepdims=True))
        return found

    def arrive(j):
        with jax.named_scope("w_pay"):
            many(landed.at[pl.ds(2 * j, 2)], pay_send, pay_recv.at[j]).wait_recv()

    for k in range(half + 2, members):
        pay_copy(k).start()
    with jax.named_scope("w_raw"):
        all_raw.wait_recv()
        for o in range(1, t):
            forward(o, core).start()
        all_keeps.wait_recv()
        for o in range(1, t):
            forward(o, lax.rem(core - o + t, t)).wait_recv()
    with jax.named_scope("raw"):
        x = raw[...].reshape((half - 1) * positions, model)
        key, _ = forget(x, [rows_in[k] for k in range(half - 1)])
        weighted[1:half] = key.reshape(half - 1, positions, width)
        values[1:half] = value(x).reshape(half - 1, positions, width)
    with jax.named_scope("w_early"):
        all_early.wait_recv()
        for c in range(1, cubes):

            @pl.when(c > cube)
            def _():
                many(cross.at[c], cross_send.at[0], cross_recv.at[c]).wait_recv()

            @pl.when(c <= cube)
            def _():
                cross[c] = jnp.zeros((members, 1, width), F32)

    with jax.named_scope("decays"):
        suffix = jnp.zeros((1, width), F32)
        for c in range(1, cubes):
            for p in range(members):
                suffix = suffix + cross[c, p]
        for p in reversed(range(members)):
            decays[p] = jnp.exp(suffix)
            suffix = suffix + early[p, 0]
    tail = half // 2 - 1
    for j in range(tail):
        arrive(j)
    with jax.named_scope("states"):
        add_up(0, members - 2, True)
    arrive(tail)
    with jax.named_scope("tail_states"):
        found = add_up(members - 2, members, False)
        reads[cube, pl.ds(mine, 1), :] = jnp.concatenate(found, axis=1)
    with jax.named_scope("sendreads"):
        for o in range(n - 1, 0, -1):
            read_copy(o).start()
    with jax.named_scope("tail_codes"):
        for h in range(heads):
            own = slice(h * head, (h + 1) * head)
            for g in range(group):
                span = slice(g * rows, (g + 1) * rows)
                most = column_most(states[h, span])
                codes[h, span], scales[g, :, own] = encode(states[h, span], most), most
        for g in range(group):

            @pl.when(keeper(g) != me)
            def _():
                scale_copy(g).start()
                state_copy(g).start()

            @pl.when(keeper(g) == me)
            def _():
                got_codes[cube] = codes[:, g * rows : (g + 1) * rows]
                got_scales[cube] = scales[g]

    source = prompt_of(me // group)
    for c in range(cubes):

        @pl.when(c * members + source != me)
        @jax.named_scope("w_states")
        def _():
            for piece, arrived in ((got_scales.at[c], scale_recv.at[c]), (got_codes.at[c], state_recv.at[c])):
                pltpu.make_async_remote_copy(
                    src_ref=piece, dst_ref=piece,
                    send_sem=read_send, recv_sem=arrived,
                    device_id=(c * members + source, core), device_id_type=MESH,
                ).wait_recv()

    for h in range(heads):
        own = slice(h * head, (h + 1) * head)
        cache_out[h] = sum(decode(got_codes[c, h], got_scales[c, :, own]) for c in range(cubes)).astype(BF16)

    with jax.named_scope("w_reads"):
        all_reads.wait_recv()
    mixed = sums[0]
    for c in range(cubes):
        mixed = mixed + reads[c]
    for h in range(heads):
        own = slice(h * head, (h + 1) * head)
        part_mixed = mixed[:, own]
        spread = lax.rsqrt(jnp.mean(part_mixed * part_mixed, axis=1, keepdims=True) + EPSILON)
        read_out[:, own] = (part_mixed * spread * sums[1, :, own]).astype(BF16)

    all_raw.wait_send()
    all_keeps.wait_send()
    all_pay.wait_send()
    for o in range(1, t):
        token_copy(o, core).wait_send()
        forward(o, core).wait_send()
    all_early.wait_send()
    for c in range(cubes - 1):

        @pl.when(c < cube)
        def _():
            many(cross.at[0], cross_send.at[c], early_recv).wait_send()

    for g in range(group):

        @pl.when(keeper(g) != me)
        def _():
            scale_copy(g).wait_send()
            state_copy(g).wait_send()

    all_reads.wait_send()


def hand_over(cache, read, cache_out, read_out, sem):
    copies = [pltpu.make_async_copy(cache, cache_out, sem.at[0]), pltpu.make_async_copy(read, read_out, sem.at[1])]
    for copy in copies:
        copy.start()
    for copy in copies:
        copy.wait()


def per_device(prompt, keep_scale, new_token, w_query, w_forget, w_value, w_outgate, floor_gap, norm_gain):
    n, t = lax.axis_size("sp"), lax.axis_size("tp")
    s_count, positions, model = prompt.shape
    head = norm_gain.shape[0]
    width = w_forget.shape[1]
    heads = width // head
    members = s_count
    cubes = n // members
    group = cubes
    rows = head // group
    sizes = (n, t, s_count, members, cubes, heads, head, rows)
    dma = pltpu.SemaphoreType.DMA
    vmem = pl.BlockSpec(memory_space=pltpu.VMEM)
    hbm = pl.BlockSpec(memory_space=pltpu.HBM)
    cache, read = pl.pallas_call(
        functools.partial(kernel, sizes),
        out_shape=(
            pltpu.VMEM((heads, rows, head), BF16),
            pltpu.VMEM((s_count, width), BF16),
        ),
        in_specs=[hbm] * 9,
        out_specs=(vmem, vmem),
        scratch_shapes=[
            pltpu.VMEM((members, positions, model), BF16),
            pltpu.VMEM((members // 2 - 1, positions, model), BF16),
            pltpu.VMEM((1,) + keep_scale.shape, F32),
            pltpu.VMEM((members // 2 - 1, 1, positions), F32),
            pltpu.VMEM((t,) + new_token.shape, BF16),
            pltpu.VMEM((model, width), BF16),
            pltpu.VMEM((model, width), BF16),
            pltpu.VMEM((2, model, width), BF16),
            pltpu.VMEM((1, width), F32),
            pltpu.VMEM((1, head), F32),
            pltpu.VMEM((members // 2, positions, 2 * width), BF16),
            pltpu.VMEM((members // 2, positions, 2 * width), BF16),
            pltpu.VMEM((members // 2, positions, width), F32),
            pltpu.VMEM((members // 2, positions, width), BF16),
            pltpu.VMEM((members, 1, width), F32),
            pltpu.VMEM((members, 2, 1, width), F32),
            pltpu.VMEM((members, 2, 1, width), F32),
            pltpu.VMEM((cubes, members, 1, width), F32),
            pltpu.VMEM((heads, head, head), F32),
            pltpu.VMEM((heads, head, head), BF16),
            pltpu.VMEM((group, 1, width), F32),
            pltpu.VMEM((cubes, heads, rows, head), BF16),
            pltpu.VMEM((cubes, 1, width), F32),
            pltpu.VMEM((cubes, s_count, width), F32),
            pltpu.VMEM((n - 1, 1, width), F32),
            pltpu.VMEM((2, s_count, width), F32),
            pltpu.VMEM((heads, head, head), F32),
            dma((7,)), dma((3,)), dma((t - 1,)),
            dma, dma, dma, dma,
            dma((t - 1,)), dma((t - 1,)),
            dma, dma((members // 4,)),
            dma((cubes - 1,)), dma((cubes,)),
            dma((t - 1,)), dma((t - 1,)),
            dma, dma,
            dma((group,)), dma((cubes,)),
            dma((group,)), dma((cubes,)),
            dma, dma,
            pltpu.SemaphoreType.REGULAR,
        ],
        compiler_params=pltpu.CompilerParams(collective_id=0, has_side_effects=True, vmem_limit_bytes=32*1024*1024),
    )(
        *(
            pltpu.with_memory_space_constraint(x, pltpu.HBM)
            for x in (
                prompt, keep_scale, new_token, w_query, w_forget, w_value, w_outgate,
                floor_gap.reshape(1, width), norm_gain.reshape(1, head),
            )
        )
    )
    return pl.pallas_call(
        hand_over,
        out_shape=(
            jax.ShapeDtypeStruct((heads, rows, head), BF16),
            jax.ShapeDtypeStruct((s_count, width), BF16),
        ),
        in_specs=[vmem, vmem],
        out_specs=(pl.BlockSpec(memory_space=pltpu.HBM), pl.BlockSpec(memory_space=pltpu.HBM)),
        scratch_shapes=[dma((2,))],
        compiler_params=pltpu.CompilerParams(vmem_limit_bytes=1024*1024),
    )(cache, read)


def solution(mesh):
    return jax.shard_map(
        per_device,
        mesh=mesh,
        in_specs=(
            P(None, "sp", None),
            P(None, "sp"),
            P(None, "tp"),
            P(None, "tp"),
            P(None, "tp"),
            P(None, "tp"),
            P(None, "tp"),
            P("tp"),
            P(),
        ),
        out_specs=(P("tp", "sp", None), P(None, "tp")),
        check_vma=False,
    )
```
